32 devices in a mesh: ep: 8 (over z, x), tp: 4 (over y, core).
Axes of the slice: x: 2, y: 2, z: 4, core: 2. Of those that a mesh axis runs over, the one named last changes fastest.
Arguments:
- tokens: bfloat16 [2048, 2048], P('ep'), may hold values from -6 to 6
- routes: int32 [2048, 2], P('ep'), may hold values from 0 to 7, all different within a row; in each aligned block of 256 rows (0 to 255, 256 to 511, ...) at most 128 rows name the same one
- router_matrix: bfloat16 [2048, 8], replicated, may hold values from -0.125 to 0.125
- cotangent: bfloat16 [2048, 2048], P('ep', 'tp'), may hold values from -3 to 3
- gate_proj: bfloat16 [8, 2048, 3584], P('ep', None, 'tp'), may hold values from -0.125 to 0.125
- up_proj: bfloat16 [8, 2048, 3584], P('ep', None, 'tp'), may hold values from -0.125 to 0.125
- down_proj: bfloat16 [8, 3584, 2048], P('ep', 'tp'), may hold values from -0.09375 to 0.09375
Outputs:
- token_grad: bfloat16 [2048, 2048], P('ep', 'tp')
- mixing_grad: float32 [2048, 2], P('ep')
- router_grad: float32 [2048, 8], P(('ep', 'tp'))
- gate_grad: bfloat16 [8, 2048, 3584], P('ep', None, 'tp')
- up_grad: bfloat16 [8, 2048, 3584], P('ep', None, 'tp')
- down_grad: bfloat16 [8, 3584, 2048], P('ep', 'tp')
The draws below stay inside these ranges and needn't reach their ends.
Inputs may be any that keep to these rules, and one draw needn't show every extreme that they name: `routes`: the two experts of a row differ. In each aligned block of 256 rows no expert is named by more than 128 rows, a bound that some block reaches; every expert is named somewhere.
All inputs are finite; a program needn't handle non-finite values.
Results may differ from the reference program's by a relative error of at most 0.019.
Values may be sent and summed in bfloat16 or wider, within the bound.
A program may use at most 128 MiB of HBM per device.

```python
import math
import jax
import jax.numpy as jnp
import numpy as np
from jax import lax

D = 2048
FF = 3584
TOP = 2
TOK_DEV = 256
EXPERTS = 8
TOKENS = 2048
CAP = 128
N_EP = 8
N_TP = 4


def steps_of(rng, extent, cuts, least, top_value):
    gain = 1.0
    for dim, shards_of in cuts:
        draws = jax.random.uniform(jax.random.fold_in(jax.random.fold_in(rng, 6), dim), (shards_of,), jnp.float32, least / len(cuts), top_value / len(cuts))
        gain = gain * jnp.repeat(jnp.exp(draws), extent[dim] // shards_of).reshape((-1,) + (1,) * (len(extent) - 1 - dim))
    return gain


def routed_block(own_key, own, number, rows, amount, top, most, slope):
    ranking = jax.random.permutation(own_key, amount)
    heavy_load, common = portions_of(amount, rows * top, most, slope, True), portions_of(amount, rows * top, most, slope, False)
    places = jnp.arange(amount)

    def named(tallies, rotation):
        used = int((tallies > 0).sum())
        fixed = max(1, used // 4)
        shifted = fixed + (places - fixed + rotation * (used - fixed)) % max(1, amount - fixed)
        return jnp.zeros((amount,), jnp.int32).at[ranking[jnp.where(places < fixed, places, shifted)]].set(jnp.asarray(tallies, jnp.int32))

    tallies = jnp.where(number % 4 == 0, named(heavy_load, number // 4), named(common, number - number // 4 - 1))
    mixed = jax.random.permutation(jax.random.fold_in(own, 3), amount)
    donor, sink = mixed[0:amount // 2 * 2:2], mixed[1:amount // 2 * 2:2]
    slack = jnp.minimum(tallies[donor] - 1, most - tallies[sink]) // 2
    slack = jnp.where((donor == ranking[0]) | (sink == ranking[0]) | (tallies[sink] == 0), 0, jnp.maximum(slack, 0))
    shifted = jax.random.randint(jax.random.fold_in(own, 4), (amount // 2,), 0, 1 << 20) % (slack + 1)
    tallies = tallies.at[donor].add(-shifted).at[sink].add(shifted)
    items = jnp.searchsorted(jnp.cumsum(tallies), jnp.arange(rows * top), side="right").astype(jnp.int32)
    table = items.reshape(top, rows).T
    table = table[jax.random.permutation(jax.random.fold_in(own, 1), rows)]
    rotation = jax.random.randint(jax.random.fold_in(own, 2), (rows, 1), 0, top)
    return jnp.take_along_axis(table, (jnp.arange(top)[None, :] + rotation) % top, axis=1)


def portions_of(number_of, total, limit, slope, full):
    weights = [(1 << 20) // math.isqrt(standing ** slope) + 1 for standing in range(1, number_of + 1)]
    largest = limit if full else min(limit, max(-(-total // number_of), total * weights[0] // sum(weights)))
    least = 1 if total - largest >= number_of - 1 else 0
    holding, surplus = [largest] + [least] * (number_of - 1), total - largest - least * (number_of - 1)
    while surplus > 0:
        movable = [i for i in range(1, number_of) if holding[i] < largest] or [i for i in range(1, number_of) if holding[i] < limit]
        whole, budget = sum([weights[i] for i in movable]), surplus
        for i in movable:
            addition = min(limit - holding[i], max(1, budget * weights[i] // whole), surplus)
            holding[i] = holding[i] + addition
            surplus = surplus - addition
    return np.array(holding)


def normal_values(own_key, dims, deviation, bound, split=(), kind=jnp.bfloat16):
    drawn = deviation * jax.random.normal(own_key, dims, jnp.float32)
    if split:
        drawn = drawn * steps_of(own_key, dims, split, -0.22, 0.18)
    return jnp.clip(drawn, -bound, bound).astype(kind)


def setup_inputs(seed: int = 0) -> dict:
    key_of = jax.random.split(jax.random.key(seed), 8)
    tokens = normal_values(key_of[0], (TOKENS, D), 1.0, 6.0, ((0, 8),))
    routes_keys = jax.random.split(jax.random.fold_in(key_of[1], 1), TOKENS // TOK_DEV)
    routes_turns = jax.random.permutation(jax.random.fold_in(key_of[1], 3), TOKENS // TOK_DEV)
    routes = jax.vmap(lambda own, number: routed_block(jax.random.fold_in(key_of[1], 2), own, number, TOK_DEV, EXPERTS, TOP, CAP, 2))(routes_keys, routes_turns).reshape((TOKENS, TOP))
    router_matrix = normal_values(key_of[2], (D, EXPERTS), D ** -0.5, 0.125)
    cotangent = normal_values(key_of[3], (TOKENS, D), 0.5, 3.0, ((0, 8), (1, 4)))
    gate_proj = normal_values(key_of[4], (EXPERTS, D, FF), D ** -0.5, 0.125, ((0, 8), (2, 4)))
    up_proj = normal_values(key_of[5], (EXPERTS, D, FF), D ** -0.5, 0.125, ((0, 8), (2, 4)))
    down_proj = normal_values(key_of[6], (EXPERTS, FF, D), FF ** -0.5, 0.09375, ((0, 8), (1, 4)))
    return {"tokens": tokens, "routes": routes, "router_matrix": router_matrix, "cotangent": cotangent, "gate_proj": gate_proj, "up_proj": up_proj, "down_proj": down_proj}


def slot_places(flat_routes, experts, capacity):
    onehot = (flat_routes[:, None] == jnp.arange(experts, dtype=jnp.int32)[None, :]).astype(jnp.int32)
    earlier = jnp.cumsum(onehot, axis=0) - onehot
    places = (flat_routes * capacity + lax.optimization_barrier(jnp.sum(earlier * onehot, axis=1))).astype(jnp.int32)
    entries = flat_routes.shape[0]
    filler = jnp.full((experts * capacity,), entries, jnp.int32).at[places].set(jnp.arange(entries, dtype=jnp.int32))
    return (places, filler)

def expert_pass(operands):
    token_rows, output_rows, mix_rows, w_gate, w_up, w_down = operands
    mix_value = mix_rows.astype(jnp.float32)
    gate_pre = jnp.dot(token_rows, w_gate, preferred_element_type=jnp.float32)
    up_pre = jnp.dot(token_rows, w_up, preferred_element_type=jnp.float32)
    gate_sig = jax.nn.sigmoid(gate_pre)
    active = gate_pre * gate_sig
    hidden = (active * up_pre).astype(jnp.bfloat16)
    back_hidden = jnp.dot(output_rows, w_down.T, preferred_element_type=jnp.float32)
    mix_part = lax.optimization_barrier(jnp.sum(hidden.astype(jnp.float32) * back_hidden, axis=1))
    scaled = mix_value[:, None] * back_hidden
    gate_back = (scaled * up_pre * gate_sig * (1.0 + gate_pre * (1.0 - gate_sig))).astype(jnp.bfloat16)
    up_back = (scaled * active).astype(jnp.bfloat16)
    out_scaled = (mix_value[:, None] * output_rows.astype(jnp.float32)).astype(jnp.bfloat16)
    gate_grad = jnp.dot(token_rows.T, gate_back, preferred_element_type=jnp.float32).astype(jnp.bfloat16)
    up_grad = jnp.dot(token_rows.T, up_back, preferred_element_type=jnp.float32).astype(jnp.bfloat16)
    down_grad = jnp.dot(hidden.T, out_scaled, preferred_element_type=jnp.float32).astype(jnp.bfloat16)
    slots = token_rows.shape[0]
    group = FF // N_TP
    gate_blocks = gate_back.astype(jnp.float32).reshape(slots, N_TP, group)
    up_blocks = up_back.astype(jnp.float32).reshape(slots, N_TP, group)
    terms = jnp.einsum('rtf,dtf->trd', gate_blocks, w_gate.astype(jnp.float32).reshape(D, N_TP, group))
    terms = terms + jnp.einsum('rtf,dtf->trd', up_blocks, w_up.astype(jnp.float32).reshape(D, N_TP, group))
    rounded = lax.optimization_barrier(terms.astype(jnp.bfloat16)).astype(jnp.float32)
    token_slots = lax.optimization_barrier(jnp.sum(rounded, axis=0)).astype(jnp.bfloat16)
    return (gate_grad, up_grad, down_grad, token_slots, mix_part)

def to_experts(rows):
    shaped = rows.reshape((N_EP, EXPERTS, CAP) + rows.shape[2:])
    return jnp.swapaxes(shaped, 0, 1).reshape((EXPERTS, N_EP * CAP) + rows.shape[2:])

def to_home(rows):
    shaped = rows.reshape((EXPERTS, N_EP, CAP) + rows.shape[2:])
    return jnp.swapaxes(shaped, 0, 1).reshape((N_EP, EXPERTS * CAP) + rows.shape[2:])

def reference(tokens, routes, router_matrix, cotangent, gate_proj, up_proj, down_proj):
    entries = TOK_DEV * TOP
    home_routes = routes.reshape(N_EP, entries)
    places, filler = jax.vmap(lambda flat: slot_places(flat, EXPERTS, CAP))(home_routes)
    occupied = filler < entries
    offsets = (jnp.arange(N_EP, dtype=jnp.int32) * TOK_DEV)[:, None]
    source = (jnp.where(occupied, filler // TOP, 0) + offsets).astype(jnp.int32)
    entry_src = (jnp.where(occupied, filler, 0) + offsets * TOP).astype(jnp.int32)
    logits = jnp.dot(tokens, router_matrix, preferred_element_type=jnp.float32)
    picked = routes[:, :, None] == jnp.arange(EXPERTS, dtype=jnp.int32)[None, None, :]
    chosen = lax.optimization_barrier(jnp.sum(jnp.where(picked, logits[:, None, :], jnp.float32(0.0)), axis=2))
    mixing = jax.nn.sigmoid(chosen - chosen[:, ::-1])
    token_slots = jnp.where(occupied[:, :, None], tokens[source], jnp.zeros((), jnp.bfloat16))
    output_slots = jnp.where(occupied[:, :, None], cotangent[source], jnp.zeros((), jnp.bfloat16))
    mix_slots = jnp.where(occupied, mixing.reshape(-1)[entry_src], jnp.float32(0.0)).astype(jnp.bfloat16)
    results = lax.map(expert_pass, (to_experts(token_slots), to_experts(output_slots), to_experts(mix_slots), gate_proj, up_proj, down_proj))
    gate_grad, up_grad, down_grad, back_slots, back_mix = results
    pick_rows = jax.vmap(lambda rows, where_at: rows[where_at])
    token_part = lax.optimization_barrier(jnp.sum(pick_rows(to_home(back_slots), places).reshape(TOKENS, TOP, D).astype(jnp.float32), axis=1))
    mixing_grad = pick_rows(to_home(back_mix), places).reshape(TOKENS, TOP)
    pairwise = mixing[:, 0] * mixing[:, 1]
    logit_grad = pairwise[:, None] * (mixing_grad - mixing_grad[:, ::-1])
    route_grad = lax.optimization_barrier(jnp.sum(jnp.where(picked, logit_grad[:, :, None], jnp.float32(0.0)), axis=1))
    router_path = jnp.dot(route_grad, router_matrix.astype(jnp.float32).T, precision=lax.Precision.HIGHEST)
    token_grad = (token_part + router_path).astype(jnp.bfloat16)
    router_grad = jnp.dot(tokens.astype(jnp.float32).T, route_grad, precision=lax.Precision.HIGHEST) * (1.0 / math.sqrt(TOKENS))
    return (token_grad, mixing_grad, router_grad, gate_grad, up_grad, down_grad)
```

```python
import math

import jax
import jax.numpy as jnp
from jax import lax
from jax.experimental import pallas as pl
from jax.experimental.pallas import tpu as pltpu
from jax.sharding import PartitionSpec as P

MESH = pl.DeviceIdType.MESH
LANES = 128
CHUNK = 256
BF = jnp.bfloat16
F32 = jnp.float32
NN = (((1,), (0,)), ((), ()))
NT = (((1,), (1,)), ((), ()))
TN = (((0,), (0,)), ((), ()))


def dot(a, b, dims=NN):
    return lax.dot_general(a, b, dims, preferred_element_type=F32)


def remote(src, dst, send, recv, ep, tp):
    return pltpu.make_async_remote_copy(
        src_ref=src,
        dst_ref=dst,
        send_sem=send,
        recv_sem=recv,
        device_id=(ep, tp),
        device_id_type=MESH,
    )


def pair(me, k, size):
    return sum((me // bit + k // bit) % 2 * bit for bit in (1 << b for b in range(size.bit_length() - 1)))


def span(start, size):
    return pl.ds(pl.multiple_of(start * size, size), size)


def each(lo, hi, action):
    def step(k, carry):
        action(k)
        return carry

    lax.fori_loop(lo, hi, step, 0)


def split(value):
    high = value.astype(BF)
    rest = value - high.astype(F32)
    middle = rest.astype(BF)
    low = (rest - middle.astype(F32)).astype(BF)
    return jnp.concatenate([high, middle, low], axis=0)


def layer_kernel(senders, rows, capacity, col, hidden, share):
    seats = 2 * rows
    width = col * seats
    per_chunk = max(1, min(senders, CHUNK // capacity))
    chunk = per_chunk * capacity
    chunks = senders // per_chunk
    half = max(senders // 2, 1)

    def body(tok_ref, cot_ref, routes_ref, router_ref, wg_hbm, wu_hbm, wd_hbm,
             tg_out, mix_out, rt_out, gg, ug, dg,
             wg, wu, wd, pick, tok_send, cot_send, mix_send, mix_in, tok_rows, cot_rows,
             hs, gb, ub, terms, mp_send, mp_got, mix_all, c_buf, y_src, y_buf, fin, home, rt_full, rt_got,
             w_sem, ep_send, ep_recv, y_send, y_recv, c_send, c_recv, m_send, m_recv,
             rc_send, rc_recv, ry_send, ry_recv, h_send, h_recv, p_send, p_recv, t_send, t_recv, r_send, r_recv):
        me = lax.axis_index("ep")
        tp = lax.axis_index("tp")
        row = tp // 2
        core = tp % 2
        partner = row * 2 + (1 - core)
        my_chunk = me // per_chunk

        def seat(step, side):
            return lax.rem(row + step + rows, rows) * 2 + side

        def peer(k):
            return pair(me, k, senders)

        barrier = pltpu.get_barrier_semaphore()
        each(1, senders, lambda k: pl.semaphore_signal(barrier, inc=1, device_id=(peer(k), tp), device_id_type=MESH))
        for k in range(1, seats):
            pl.semaphore_signal(barrier, inc=1, device_id=(me, lax.rem(tp + k, seats)), device_id_type=MESH)

        loads = [pltpu.make_async_copy(src, dst, w_sem.at[i])
                 for i, (src, dst) in enumerate(((wg_hbm, wg), (wu_hbm, wu), (wd_hbm, wd)))]
        for load in loads:
            load.start()

        ids = lax.broadcasted_iota(jnp.int32, (senders, tok_ref.shape[0]), 0)
        is_first = ids == routes_ref[0:1, :]
        is_second = ids == routes_ref[1:2, :]
        member = jnp.where(is_first | is_second, 1.0, 0.0)
        home_rows = tok_ref.shape[0]
        earlier = lax.broadcasted_iota(jnp.int32, (home_rows, home_rows), 0) < lax.broadcasted_iota(
            jnp.int32, (home_rows, home_rows), 1)
        rank = dot(member.astype(BF), jnp.where(earlier, 1.0, 0.0).astype(BF))
        place = jnp.where(member > 0.0, rank, -1.0)
        slot_ids = lax.broadcasted_iota(jnp.int32, (capacity, home_rows), 0).astype(F32)
        for e in range(senders):
            pick[e * capacity:(e + 1) * capacity, :] = jnp.where(slot_ids == place[e:e + 1, :], 1.0, 0.0).astype(BF)

        logits = dot(router_ref[...], tok_ref[...], NT)
        chosen_first = jnp.sum(jnp.where(is_first, logits, 0.0), axis=0, keepdims=True)
        chosen_second = jnp.sum(jnp.where(is_second, logits, 0.0), axis=0, keepdims=True)
        mix_first = 1.0 / (1.0 + jnp.exp(chosen_second - chosen_first))
        mix_second = 1.0 / (1.0 + jnp.exp(chosen_first - chosen_second))
        mix_value = jnp.where(is_first, mix_first, jnp.where(is_second, mix_second, 0.0)).astype(BF)
        for e in range(senders):
            mix_send[e, :, 0:capacity] = dot(mix_value, pick[e * capacity:(e + 1) * capacity, :], NT)
        mix_in[me] = mix_send[me]

        cot_send[...] = dot(pick[...], cot_ref[...]).astype(BF)
        for r in range(rows):
            tok_send[r] = dot(pick[...], tok_ref[:, span(seat(r, core), col)]).astype(BF)
        own = span(me, capacity)
        tok_rows[own, :] = dot(pick[own, :], tok_ref[...]).astype(BF)
        cot_rows[own, span(tp, col)] = cot_send[own, :]

        pl.semaphore_wait(barrier, senders - 1 + seats - 1)

        arrays = (tok_rows, cot_rows)

        def piece(array, block, tp_col):
            return array.at[span(block, capacity), span(tp_col, col)]

        mine = [(1, 0)]
        far = [(1, 0), (0, 0)]
        near = far + [(0, j) for j in range(1, rows)]
        far_hops = [(a, j) for j in range(1, rows) for a in (1, 0)]
        near_hops = [(1, j) for j in range(1, rows)]

        def ep_copy(i, dest, block):
            array, which = near[i]
            source = (tok_send.at[which] if array == 0 else cot_send).at[span(dest, capacity), :]
            return remote(source, piece(arrays[array], block, seat(which, core)),
                          ep_send.at[i, dest], ep_recv.at[i, block], dest, tp)

        def mix_copy(dest, block):
            return remote(mix_send.at[dest], mix_in.at[block], m_send.at[dest], m_recv.at[block], dest, tp)

        def y_copy(array, step, block):
            at = piece(arrays[array], block, tp)
            return remote(at, at, y_send.at[array, step, block], y_recv.at[array, step, block], me, seat(step, core))

        def y_arrival(array, step, block):
            at = piece(arrays[array], block, seat(-step, core))
            return remote(at, at, y_send.at[array, step, block], y_recv.at[array, step, block], me, seat(step, core))

        def c_copy(array, step, block):
            at = piece(arrays[array], block, seat(step, core))
            return remote(at, at, c_send.at[array, step + rows, block], c_recv.at[array, step + rows, block],
                          me, partner)

        def c_arrival(array, step, block):
            at = piece(arrays[array], block, seat(step, 1 - core))
            return remote(at, at, c_send.at[array, step + rows, block], c_recv.at[array, step + rows, block],
                          me, partner)

        def send_to(count):
            def action(k):
                dest = peer(k)
                mix_copy(dest, me).start()
                for i in range(count):
                    ep_copy(i, dest, me).start()

            return action

        each(1, half, send_to(len(near)))
        each(half, senders, send_to(len(far)))

        def spread(block, items, hops):
            for array, step in hops:
                y_copy(array, step, block).start()
            for array, step in items:
                c_copy(array, step, block).start()

        def take(items, hops):
            def action(j):
                block = peer(j)
                for i in range(len(items)):
                    ep_copy(i, block, block).wait_recv()
                spread(block, items, hops)

            return action

        def pass_on(hops):
            def action(j):
                block = peer(j)
                for array, step in hops:
                    y_arrival(array, step, block).wait_recv()
                    c_copy(array, -step, block).start()

            return action

        def settle(items, hops):
            def action(j):
                block = peer(j)
                for array, step in items + [(a, -s) for a, s in hops]:
                    c_arrival(array, step, block).wait_recv()

            return action

        def arrive_mix(j):
            mix_copy(peer(j), peer(j)).wait_recv()

        def home_copy(dest, slot):
            return remote(fin.at[span(dest, capacity), :], home.at[span(slot, capacity), :],
                          h_send.at[dest], h_recv.at[slot], dest, tp)

        def part_copy(dest, slot):
            return remote(mp_send.at[dest], mp_got.at[slot], p_send.at[dest], p_recv.at[slot], dest, tp)

        def rc_copy(step, block):
            return remote(piece(terms, block, seat(step, 1 - core)), c_buf.at[step, span(block, capacity), :],
                          rc_send.at[step, block], rc_recv.at[step, block], me, partner)

        def ry_copy(step, block):
            return remote(y_src.at[step - 1, span(block, capacity), :], y_buf.at[step - 1, span(block, capacity), :],
                          ry_send.at[step, block], ry_recv.at[step, block], me, seat(step, core))

        def start_back(j):
            block = peer(j)
            for step in list(range(1, rows)) + [0]:
                rc_copy(step, block).start()

        def first(j):
            block = peer(j)
            at = span(block, capacity)
            for step in range(1, rows):
                rc_copy(step, block).wait_recv()
                y_src[step - 1, at, :] = (
                    terms[at, span(seat(step, core), col)].astype(F32) + c_buf[step, at, :].astype(F32)
                ).astype(BF)
                ry_copy(step, block).start()

        def second(j):
            block = peer(j)
            at = span(block, capacity)
            rc_copy(0, block).wait_recv()
            value = terms[at, span(tp, col)].astype(F32) + c_buf[0, at, :].astype(F32)
            for step in range(1, rows):
                ry_copy(step, block).wait_recv()
                value = value + y_buf[step - 1, at, :].astype(F32)
            fin[at, :] = value.astype(BF)

            @pl.when(j > 0)
            def _():
                home_copy(block, me).start()

        diagonal = lax.broadcasted_iota(jnp.int32, (capacity, capacity), 0) == lax.broadcasted_iota(
            jnp.int32, (capacity, capacity), 1)

        def to_column(values):
            return jnp.sum(jnp.where(diagonal, values, 0.0), axis=1, keepdims=True)

        def to_row(values):
            return jnp.sum(jnp.where(diagonal, values, 0.0), axis=0, keepdims=True)

        def forward(which):
            at = span(which, chunk)
            mixes = jnp.concatenate(
                [to_column(mix_in[which * per_chunk + i, pl.ds(me, 1), :][:, 0:capacity]) for i in range(per_chunk)],
                axis=0)
            x = tok_rows[at, :]
            dy = cot_rows[at, :]
            total = jnp.zeros((chunk, 1), F32)
            for n0 in range(0, hidden, CHUNK):
                n = min(CHUNK, hidden - n0)
                gate = dot(x, wg[:, n0:n0 + n])
                up = dot(x, wu[:, n0:n0 + n])
                back = dot(dy, wd[n0:n0 + n, :], NT)
                sig = 1.0 / (1.0 + jnp.exp(-gate))
                active = gate * sig
                inner = active * up
                total = total + jnp.sum(inner * back, axis=1, keepdims=True)
                scaled = mixes * back
                gb[at, n0:n0 + n] = (scaled * up * sig * (1.0 + gate * (1.0 - sig))).astype(BF)
                ub[at, n0:n0 + n] = (scaled * active).astype(BF)
                hs[at, n0:n0 + n] = (mixes * inner).astype(BF)
            for i in range(per_chunk):
                line = to_row(total[i * capacity:(i + 1) * capacity, :])
                mp_send[which * per_chunk + i, :, 0:capacity] = jnp.broadcast_to(line, (8, capacity))

        def backward(which):
            at = span(which, chunk)
            gate_back = gb[at, :]
            up_back = ub[at, :]
            for d0 in range(0, width, 512):
                terms[at, d0:d0 + 512] = (
                    dot(gate_back, wg[d0:d0 + 512, :], NT) + dot(up_back, wu[d0:d0 + 512, :], NT)
                ).astype(BF)

        def order(s):
            if chunks != 4:
                return s
            return pair(s, s // 2 * ((my_chunk + my_chunk // 2) % 2), chunks)

        spread(me, mine, near_hops)

        def step_of(s):
            k = order(s)
            lo = k * per_chunk
            hi = lo + per_chunk
            near_lo, near_hi = jnp.maximum(lo, 1), jnp.minimum(hi, half)
            far_lo = jnp.maximum(lo, half)
            own_hi = jnp.where(s == 0, 1, 0)
            each(near_lo, near_hi, take(near, near_hops))
            each(far_lo, hi, take(far, far_hops))

            @pl.when(s > 0)
            def _():
                before = order(s - 1) * per_chunk
                each(before, before + per_chunk, second)

            each(0, own_hi, pass_on(near_hops))
            each(near_lo, near_hi, pass_on(near_hops))
            each(far_lo, hi, pass_on(far_hops))
            each(0, own_hi, settle(mine, near_hops))
            each(near_lo, near_hi, settle(near, near_hops))
            each(far_lo, hi, settle(far, far_hops))
            each(jnp.maximum(lo, 1), hi, arrive_mix)

            @pl.when(s == 0)
            def _():
                for load in loads:
                    load.wait()

            which = pair(my_chunk, k, chunks)
            forward(which)
            each(jnp.maximum(lo, 1), hi, lambda j: part_copy(peer(j), me).start())
            backward(which)
            each(lo, hi, start_back)
            each(lo, hi, first)

        each(0, chunks, step_of)
        mp_got[me] = mp_send[me]

        def gate_up(i):
            at = span(i, CHUNK)
            x = tok_rows[:, at]
            gg[at, :] = dot(x, gb[...], TN).astype(BF)
            ug[at, :] = dot(x, ub[...], TN).astype(BF)

        def down(i):
            at = span(i, LANES)
            dg[at, :] = dot(hs[:, at], cot_rows[...], TN).astype(BF)

        parts = width // CHUNK
        last = order(chunks - 1) * per_chunk
        middle = last + (per_chunk + 1) // 2
        each(0, parts // 2, gate_up)
        each(last, middle, second)
        each(parts // 2, parts * 3 // 4, gate_up)
        each(middle, last + per_chunk, second)
        each(parts * 3 // 4, parts, gate_up)

        each(1, senders, lambda j: part_copy(peer(j), peer(j)).wait_recv())
        mix_all[0] = mp_got[...]

        def t_copy(k):
            return remote(mp_got, mix_all.at[k], t_send.at[k], t_recv.at[k], me, lax.rem(tp + k, seats))

        for k in range(1, seats):
            t_copy(k).start()
        down_parts = hidden // LANES
        each(0, (down_parts + 1) // 2, down)
        for k in range(1, seats):
            t_copy(k).wait()

        slot_mix = jnp.sum(mix_all[...], axis=0)
        grads = []
        for e in range(senders):
            column = to_column(slot_mix[e, 0:1, 0:capacity])
            chosen = pick[e * capacity:(e + 1) * capacity, :].astype(F32)
            grads.append(jnp.sum(column * chosen, axis=0, keepdims=True))
        grads = jnp.concatenate(grads, axis=0)
        mg_first = jnp.sum(jnp.where(is_first, grads, 0.0), axis=0, keepdims=True)
        mg_second = jnp.sum(jnp.where(is_second, grads, 0.0), axis=0, keepdims=True)
        mix_out[0:1, :] = mg_first
        mix_out[1:2, :] = mg_second
        lg_first = mix_first * mix_second * (mg_first - mg_second)
        route_grad = split(jnp.where(is_first, lg_first, jnp.where(is_second, -lg_first, 0.0)))
        raw = dot(route_grad, tok_ref[...])
        norm_scale = 1.0 / math.sqrt(home_rows * senders)
        rt_full[...] = (raw[0:senders] + raw[senders:2 * senders] + raw[2 * senders:]) * norm_scale

        def rt_cols(dest):
            return span((dest * seats + tp) * share // LANES, LANES)

        def r_copy(dest, slot):
            return remote(rt_full.at[:, rt_cols(dest)], rt_got.at[slot], r_send.at[dest], r_recv.at[slot], dest, tp)

        each(1, senders, lambda k: r_copy(peer(k), me).start())
        rt_got[me] = rt_full[:, rt_cols(me)]
        each((down_parts + 1) // 2, down_parts, down)

        home[own, :] = fin[own, :]
        each(1, senders, lambda k: home_copy(peer(k), peer(k)).wait_recv())
        cols = router_ref[:, span(tp, col)]
        tg_out[...] = (
            dot(pick[...], home[...], TN) + dot(route_grad, jnp.concatenate([cols, cols, cols], axis=0), TN)
        ).astype(BF)
        each(1, senders, lambda k: r_copy(peer(k), peer(k)).wait_recv())
        rt_out[...] = jnp.sum(rt_got[...], axis=0)

        def close(items, hops):
            def action(j):
                block = peer(j)
                for array, step in items + [(a, -s) for a, s in hops]:
                    c_copy(array, step, block).wait_send()
                for array, step in hops:
                    y_copy(array, step, block).wait_send()

            return action

        close(mine, near_hops)(0)
        each(1, half, close(near, near_hops))
        each(half, senders, close(far, far_hops))

        def close_back(j):
            block = peer(j)
            for step in range(rows):
                rc_copy(step, block).wait_send()
            for step in range(1, rows):
                ry_copy(step, block).wait_send()

        each(0, senders, close_back)

        def close_sends(count):
            def action(k):
                dest = peer(k)
                for i in range(count):
                    ep_copy(i, dest, me).wait_send()
                mix_copy(dest, me).wait_send()
                part_copy(dest, me).wait_send()
                home_copy(dest, me).wait_send()
                r_copy(dest, me).wait_send()

            return action

        each(1, half, close_sends(len(near)))
        each(half, senders, close_sends(len(far)))

    return body


def layer(tokens, cotangent, routes, router, w_gate, w_up, w_down):
    home_rows, width = tokens.shape
    senders = router.shape[0]
    seats = lax.axis_size("tp")
    rows = seats // 2
    col = width // seats
    hidden = w_gate.shape[1]
    capacity = home_rows * routes.shape[0] * 2 // senders
    slots = senders * capacity
    share = width // (senders * seats)
    vmem = pl.BlockSpec(memory_space=pltpu.VMEM)
    hbm = pl.BlockSpec(memory_space=pl.ANY)
    dma = pltpu.SemaphoreType.DMA

    def buf(shape, dtype=BF):
        return pltpu.VMEM(shape, dtype)

    return pl.pallas_call(
        layer_kernel(senders, rows, capacity, col, hidden, share),
        out_shape=(
            jax.ShapeDtypeStruct((home_rows, col), BF),
            jax.ShapeDtypeStruct((2, home_rows), F32),
            jax.ShapeDtypeStruct((senders, LANES), F32),
            jax.ShapeDtypeStruct((width, hidden), BF),
            jax.ShapeDtypeStruct((width, hidden), BF),
            jax.ShapeDtypeStruct((hidden, width), BF),
        ),
        in_specs=[vmem] * 4 + [hbm] * 3,
        out_specs=[vmem] * 6,
        scratch_shapes=[
            buf((width, hidden)), buf((width, hidden)), buf((hidden, width)),
            buf((slots, home_rows)), buf((rows, slots, col)), buf((slots, col)),
            buf((senders, senders, LANES), F32), buf((senders, senders, LANES), F32),
            buf((slots, width)), buf((slots, width)),
            buf((slots, hidden)), buf((slots, hidden)), buf((slots, hidden)), buf((slots, width)),
            buf((senders, 8, LANES), F32), buf((senders, 8, LANES), F32), buf((seats, senders, 8, LANES), F32),
            buf((rows, slots, col)), buf((rows - 1, slots, col)), buf((rows - 1, slots, col)),
            buf((slots, col)), buf((slots, col)),
            buf((senders, width), F32), buf((senders, senders, LANES), F32),
            dma((3,)),
            dma((1 + rows, senders)), dma((1 + rows, senders)),
            dma((2, rows, senders)), dma((2, rows, senders)),
            dma((2, 2 * rows, senders)), dma((2, 2 * rows, senders)),
            dma((senders,)), dma((senders,)),
            dma((rows, senders)), dma((rows, senders)),
            dma((rows, senders)), dma((rows, senders)),
            dma((senders,)), dma((senders,)),
            dma((senders,)), dma((senders,)),
            dma((seats,)), dma((seats,)),
            dma((senders,)), dma((senders,)),
        ],
        compiler_params=pltpu.CompilerParams(has_side_effects=True, collective_id=0, vmem_limit_bytes=60 << 20),
        name="layer",
    )(tokens, cotangent, routes, router, w_gate, w_up, w_down)


def local(tokens, routes, router_matrix, cotangent, gate_proj, up_proj, down_proj):
    ep_size = lax.axis_size("ep")
    tp_size = lax.axis_size("tp")
    token_grad, mixing, router_rows, gate_grad, up_grad, down_grad = layer(
        tokens, cotangent, routes.T, router_matrix.T, gate_proj[0], up_proj[0], down_proj[0]
    )
    share = tokens.shape[1] // (ep_size * tp_size)
    start = (lax.axis_index("ep") * tp_size + lax.axis_index("tp")) * share % LANES
    router_grad = lax.dynamic_slice_in_dim(router_rows, start, share, 1).T
    return (token_grad, mixing.T, router_grad, gate_grad[None], up_grad[None], down_grad[None])


def solution(mesh):
    return jax.shard_map(
        local,
        mesh=mesh,
        in_specs=(
            P("ep", None),
            P("ep", None),
            P(),
            P("ep", "tp"),
            P("ep", None, "tp"),
            P("ep", None, "tp"),
            P("ep", "tp", None),
        ),
        out_specs=(
            P("ep", "tp"),
            P("ep", None),
            P(("ep", "tp"), None),
            P("ep", None, "tp"),
            P("ep", None, "tp"),
            P("ep", "tp", None),
        ),
        check_vma=False,
    )
```

```python
import math

import jax
import jax.numpy as jnp
from jax import lax
from jax.experimental import pallas as pl
from jax.experimental.pallas import tpu as pltpu
from jax.sharding import PartitionSpec as P

MESH = pl.DeviceIdType.MESH
LANES = 128
CHUNK = 256
OUTER_TAKES = (2, 4, 4, 4, 4, 6, 7, 8, 8, 8, 8, 8, 8, 8, 8, 8, 8)
INNER_TAKES = (2, 4, 4, 4, 4, 7, 8, 8, 8, 8, 8, 8, 8, 8, 8, 8, 8)
BF = jnp.bfloat16
F32 = jnp.float32
NN = (((1,), (0,)), ((), ()))
NT = (((1,), (1,)), ((), ()))
TN = (((0,), (0,)), ((), ()))


def dot(a, b, dims=NN):
    return lax.dot_general(a, b, dims, preferred_element_type=F32)


def remote(src, dst, send, recv, ep, tp):
    return pltpu.make_async_remote_copy(
        src_ref=src,
        dst_ref=dst,
        send_sem=send,
        recv_sem=recv,
        device_id=(ep, tp),
        device_id_type=MESH,
    )


def pair(me, k, size):
    return sum((me // bit + k // bit) % 2 * bit for bit in (1 << b for b in range(size.bit_length() - 1)))


def span(start, size):
    return pl.ds(pl.multiple_of(start * size, size), size)


def each(lo, hi, action):
    def step(k, carry):
        action(k)
        return carry

    lax.fori_loop(lo, hi, step, 0)


def split(value):
    high = value.astype(BF)
    rest = value - high.astype(F32)
    middle = rest.astype(BF)
    low = (rest - middle.astype(F32)).astype(BF)
    return jnp.concatenate([high, middle, low], axis=0)


def layer_kernel(senders, rows, capacity, col, hidden, share):
    seats = 2 * rows
    width = col * seats
    per_chunk = max(1, min(senders, CHUNK // capacity))
    chunk = per_chunk * capacity
    chunks = senders // per_chunk
    half = max(senders // 2, 1)

    def body(tok_hbm, cot_hbm, routes_hbm, router_hbm, wg_hbm, wu_hbm, wd_hbm,
             tg_out, mix_out, rt_out, gg, ug, dg,
             tok_ref, cot_ref, routes_ref, router_ref, wg, wu, wd, pick, tok_send, cot_send, cot_raw, cot_more, mix_send, mix_in, tok_rows, cot_rows,
             hs, gb, ub, terms, mp_send, mp_got, mix_all, c_buf, y_buf, home, rt_full, rt_got,
             w_sem, raw_send, raw_recv, ep_send, ep_recv, y_send, y_recv, c_send, c_recv, m_send, m_recv,
             rc_send, rc_recv, ry_send, ry_recv, h_send, h_recv, p_send, p_recv, t_send, t_recv, r_send, r_recv):
        me = lax.axis_index("ep")
        tp = lax.axis_index("tp")
        row = tp // 2
        core = tp % 2
        partner = row * 2 + (1 - core)
        my_chunk = me // per_chunk

        def seat(step, side):
            return lax.rem(row + step + rows, rows) * 2 + side

        def peer(k):
            return pair(me, k, senders)

        def raw_copy(step):
            return remote(cot_ref, cot_raw.at[step - 1], raw_send.at[step], raw_recv.at[step], me, seat(step, core))

        barrier = pltpu.get_barrier_semaphore()
        each(1, senders, lambda k: pl.semaphore_signal(barrier, inc=1, device_id=(peer(k), tp), device_id_type=MESH))
        for k in range(1, seats):
            pl.semaphore_signal(barrier, inc=1, device_id=(me, lax.rem(tp + k, seats)), device_id_type=MESH)

        loads = [pltpu.make_async_copy(src, dst, w_sem.at[i])
                 for i, (src, dst) in enumerate((
                     (routes_hbm, routes_ref), (tok_hbm, tok_ref), (router_hbm, router_ref), (cot_hbm, cot_ref),
                     (wg_hbm, wg), (wu_hbm, wu), (wd_hbm, wd)))]
        for load in loads:
            load.start()
        loads[0].wait()
        loads[3].wait()
        pl.semaphore_wait(barrier, senders - 1 + seats - 1)
        for step in range(1, rows):
            raw_copy(step).start()

        ids = lax.broadcasted_iota(jnp.int32, (senders, tok_ref.shape[0]), 0)
        is_first = ids == routes_ref[0:1, :]
        is_second = ids == routes_ref[1:2, :]
        member = jnp.where(is_first | is_second, 1.0, 0.0)
        home_rows = tok_ref.shape[0]
        earlier = lax.broadcasted_iota(jnp.int32, (home_rows, home_rows), 0) < lax.broadcasted_iota(
            jnp.int32, (home_rows, home_rows), 1)
        rank = dot(member.astype(BF), jnp.where(earlier, 1.0, 0.0).astype(BF))
        place = jnp.where(member > 0.0, rank, -1.0)
        slot_ids = lax.broadcasted_iota(jnp.int32, (capacity, home_rows), 0).astype(F32)
        for e in range(senders):
            pick[e * capacity:(e + 1) * capacity, :] = jnp.where(slot_ids == place[e:e + 1, :], 1.0, 0.0).astype(BF)

        loads[1].wait()

        def choose_rows(i):
            at = span(i, CHUNK)
            cot_send[at, :] = dot(pick[at, :], cot_ref[...]).astype(BF)
            for r in range(rows):
                tok_send[r, at, :] = dot(pick[at, :], tok_ref[:, span(seat(r, core), col)]).astype(BF)

        each(0, senders * capacity // CHUNK, choose_rows)
        own = span(me, capacity)
        tok_rows[own, :] = dot(pick[own, :], tok_ref[...]).astype(BF)
        cot_rows[own, span(tp, col)] = cot_send[own, :]

        arrays = (tok_rows, cot_rows)

        def piece(array, block, tp_col):
            return array.at[span(block, capacity), span(tp_col, col)]

        mine = [(1, -j) for j in range(rows)]
        far = [(1, 0), (0, 0)]
        early = far + [(0, j) for j in range(1, rows)]
        near = early + [(1, -j) for j in range(1, rows)]
        far_hops = [(a, j) for j in range(1, rows) for a in (1, 0)]
        near_first = me // half * half

        def ep_copy(i, dest, block):
            array, which = near[i]
            if array == 1 and which < 0:
                source = cot_more.at[-which - 1, span(dest - near_first, capacity), :]
            else:
                source = (tok_send.at[which] if array == 0 else cot_send).at[span(dest, capacity), :]
            return remote(source, piece(arrays[array], block, seat(which, core)),
                          ep_send.at[i, dest], ep_recv.at[i, block], dest, tp)

        def mix_copy(dest, block):
            return remote(mix_send.at[dest], mix_in.at[block], m_send.at[dest], m_recv.at[block], dest, tp)

        def y_copy(array, step, block):
            at = piece(arrays[array], block, tp)
            return remote(at, at, y_send.at[array, step, block], y_recv.at[array, step, block], me, seat(step, core))

        def y_arrival(array, step, block):
            at = piece(arrays[array], block, seat(-step, core))
            return remote(at, at, y_send.at[array, step, block], y_recv.at[array, step, block], me, seat(step, core))

        def c_copy(array, step, block):
            at = piece(arrays[array], block, seat(step, core))
            return remote(at, at, c_send.at[array, step + rows, block], c_recv.at[array, step + rows, block],
                          me, partner)

        def c_arrival(array, step, block):
            at = piece(arrays[array], block, seat(step, 1 - core))
            return remote(at, at, c_send.at[array, step + rows, block], c_recv.at[array, step + rows, block],
                          me, partner)

        inner = (my_chunk + my_chunk // 2) % 2

        def choose(s, values):
            return sum(jnp.where(s == i, v, 0) for i, v in enumerate(values))

        def order(s):
            if chunks != 4:
                return s
            return jnp.where(inner == 1, choose(s, (3, 1, 0, 2)), choose(s, (0, 2, 1, 3)))

        def send(lo, hi):
            def action(k):
                for i in range(lo, hi):
                    ep_copy(i, peer(k), me).start()

            return action

        def send_far(on):
            flip = inner if chunks == 4 else 0
            for s in range(half // per_chunk, chunks):
                start = pair(s, flip, chunks) * per_chunk
                each(start, start + per_chunk * on, send(0, len(far)))

        c_copy(1, 0, me).start()
        each(1, half, send(0, len(early)))
        loads[2].wait()
        logits = dot(router_ref[...], tok_ref[...], NT)
        chosen_first = jnp.sum(jnp.where(is_first, logits, 0.0), axis=0, keepdims=True)
        chosen_second = jnp.sum(jnp.where(is_second, logits, 0.0), axis=0, keepdims=True)
        mix_first = 1.0 / (1.0 + jnp.exp(chosen_second - chosen_first))
        mix_second = 1.0 / (1.0 + jnp.exp(chosen_first - chosen_second))
        mix_value = jnp.where(is_first, mix_first, jnp.where(is_second, mix_second, 0.0)).astype(BF)
        for e in range(senders):
            mix_send[e, :, 0:capacity] = dot(mix_value, pick[e * capacity:(e + 1) * capacity, :], NT)
        mix_in[me] = mix_send[me]
        each(1, senders, lambda k: mix_copy(peer(k), me).start())
        send_far(inner)
        for step in range(1, rows):
            raw_copy(step).wait_recv()
            for n0 in range(0, half * capacity, CHUNK):
                cot_more[step - 1, n0:n0 + CHUNK, :] = dot(
                    pick[pl.ds(pl.multiple_of(near_first * capacity + n0, capacity), CHUNK), :], cot_raw[step - 1]
                ).astype(BF)
            cot_rows[own, span(seat(-step, core), col)] = cot_more[step - 1, span(me - near_first, capacity), :]
            c_copy(1, -step, me).start()
        each(1, half, send(len(early), len(near)))
        send_far(1 - inner)

        def take(items, hops):
            def action(j):
                block = peer(j)
                for i, (array, step) in enumerate(items):
                    ep_copy(i, block, block).wait_recv()
                    for a, hop in hops:
                        if a == array and step == 0:
                            y_copy(array, hop, block).start()
                    c_copy(array, step, block).start()

            return action

        def pass_on(hops):
            def action(j):
                block = peer(j)
                for array, step in hops:
                    y_arrival(array, step, block).wait_recv()
                    c_copy(array, -step, block).start()

            return action

        def settle(items, hops):
            def action(j):
                block = peer(j)
                for array, step in items + [(a, -s) for a, s in hops]:
                    c_arrival(array, step, block).wait_recv()

            return action

        def arrive_mix(j):
            mix_copy(peer(j), peer(j)).wait_recv()

        def home_copy(dest, slot):
            return remote(piece(terms, dest, tp), home.at[span(slot, capacity), :],
                          h_send.at[dest], h_recv.at[slot], dest, tp)

        def part_copy(dest, slot):
            return remote(mp_send.at[dest], mp_got.at[slot], p_send.at[dest], p_recv.at[slot], dest, tp)

        def rc_copy(step, block):
            return remote(piece(terms, block, seat(step, 1 - core)), c_buf.at[step, span(block, capacity), :],
                          rc_send.at[step, block], rc_recv.at[step, block], me, partner)

        def ry_copy(step, block):
            return remote(piece(terms, block, seat(step, core)), y_buf.at[step - 1, span(block, capacity), :],
                          ry_send.at[step, block], ry_recv.at[step, block], me, seat(step, core))

        def start_back(j):
            block = peer(j)
            for step in range(1, rows):
                rc_copy(step, block).start()

        def rest_back(j):
            rc_copy(0, peer(j)).start()

        def first(j):
            block = peer(j)
            at = span(block, capacity)
            for step in range(1, rows):
                rc_copy(step, block).wait_recv()
                cols = span(seat(step, core), col)
                terms[at, cols] = (terms[at, cols].astype(F32) + c_buf[step, at, :].astype(F32)).astype(BF)
                ry_copy(step, block).start()

        def second(j):
            block = peer(j)
            at = span(block, capacity)
            rc_copy(0, block).wait_recv()
            value = terms[at, span(tp, col)].astype(F32) + c_buf[0, at, :].astype(F32)
            for step in range(1, rows):
                ry_copy(step, block).wait_recv()
                value = value + y_buf[step - 1, at, :].astype(F32)
            terms[at, span(tp, col)] = value.astype(BF)

            @pl.when(j > 0)
            def _():
                home_copy(block, me).start()

        diagonal = lax.broadcasted_iota(jnp.int32, (capacity, capacity), 0) == lax.broadcasted_iota(
            jnp.int32, (capacity, capacity), 1)

        def to_column(values):
            return jnp.sum(jnp.where(diagonal, values, 0.0), axis=1, keepdims=True)

        def to_row(values):
            return jnp.sum(jnp.where(diagonal, values, 0.0), axis=0, keepdims=True)

        def forward(which):
            at = span(which, chunk)
            mixes = jnp.concatenate(
                [to_column(mix_in[which * per_chunk + i, pl.ds(me, 1), :][:, 0:capacity]) for i in range(per_chunk)],
                axis=0)
            x = tok_rows[at, :]
            dy = cot_rows[at, :]
            total = jnp.zeros((chunk, 1), F32)
            for n0 in range(0, hidden, CHUNK):
                n = min(CHUNK, hidden - n0)
                gate = dot(x, wg[:, n0:n0 + n])
                up = dot(x, wu[:, n0:n0 + n])
                back = dot(dy, wd[n0:n0 + n, :], NT)
                sig = 1.0 / (1.0 + jnp.exp(-gate))
                active = gate * sig
                inner = active * up
                total = total + jnp.sum(inner * back, axis=1, keepdims=True)
                scaled = mixes * back
                gb[at, n0:n0 + n] = (scaled * up * sig * (1.0 + gate * (1.0 - sig))).astype(BF)
                ub[at, n0:n0 + n] = (scaled * active).astype(BF)
                hs[at, n0:n0 + n] = (mixes * inner).astype(BF)
            for i in range(per_chunk):
                line = to_row(total[i * capacity:(i + 1) * capacity, :])
                mp_send[which * per_chunk + i, :, 0:capacity] = jnp.broadcast_to(line, (8, capacity))

        def backward(which):
            at = span(which, chunk)
            gate_back = gb[at, :]
            up_back = ub[at, :]
            for d0 in range(0, width, 512):
                terms[at, d0:d0 + 512] = (
                    dot(gate_back, wg[d0:d0 + 512, :], NT) + dot(up_back, wu[d0:d0 + 512, :], NT)
                ).astype(BF)

        def ranged(own_action, near_action, far_action):
            def run(lo, hi):
                if own_action is not None:
                    each(lo, jnp.minimum(hi, 1), own_action)
                each(jnp.maximum(lo, 1), jnp.minimum(hi, half), near_action)
                each(jnp.maximum(lo, half), hi, far_action)

            return run

        take_range = ranged(None, take(near, []), take(far, far_hops))
        settle_range = ranged(settle(mine, []), settle(near, []), settle(far, far_hops))
        part = (per_chunk + 1) // 2

        def take_halves(lo, hi):
            def one(h):
                start = order(h // 2) * per_chunk + h % 2 * part
                take_range(start, start + part)

            each(lo, hi, one)

        def taken(s, point):
            def of(table):
                return choose(s, [table[4 * i + point] for i in range(4)])

            return jnp.where(inner == 1, of(INNER_TAKES), of(OUTER_TAKES))

        def take_point(s, point):
            take_halves(taken(s, point - 1), taken(s, point))

        take_halves(0, 2)

        def halves(first_step):
            return [span(pair(my_chunk, order(s), chunks), chunk) for s in range(first_step, first_step + chunks // 2)]

        def joined(ref, first_step, cols):
            return jnp.concatenate([ref[at, cols] for at in halves(first_step)], axis=0)

        def gate_up_early(i):
            at = span(i, CHUNK)
            x = joined(tok_rows, 0, at)
            gg[at, :] = dot(x, joined(gb, 0, slice(None)), TN).astype(BF)
            ug[at, :] = dot(x, joined(ub, 0, slice(None)), TN).astype(BF)

        def gate_up(i):
            at = span(i, CHUNK)
            x = joined(tok_rows, chunks // 2, at)
            gg[at, :] = (gg[at, :].astype(F32) + dot(x, joined(gb, chunks // 2, slice(None)), TN)).astype(BF)
            ug[at, :] = (ug[at, :].astype(F32) + dot(x, joined(ub, chunks // 2, slice(None)), TN)).astype(BF)

        def step_of(s):
            lo = order(s) * per_chunk
            hi = lo + per_chunk
            before = order(jnp.maximum(s - 1, 0)) * per_chunk
            earlier_chunk = order(jnp.maximum(s - 2, 0)) * per_chunk
            which = pair(my_chunk, order(s), chunks)

            each(jnp.maximum(lo, half), hi, pass_on(far_hops))
            settle_range(lo, hi)
            each(jnp.maximum(lo, 1), hi, arrive_mix)

            @pl.when(s == 0)
            def _():
                for load in loads[4:]:
                    load.wait()

            forward(which)
            each(jnp.maximum(lo, 1), hi, lambda j: part_copy(peer(j), me).start())
            take_point(s, 1)
            each(earlier_chunk, earlier_chunk + jnp.where(s > 1, per_chunk, 0), second)
            backward(which)
            each(lo, hi, start_back)
            each(lo, hi, rest_back)
            take_point(s, 2)
            each(0, jnp.where(s == chunks // 2 - 1, width // CHUNK, 0), gate_up_early)
            take_point(s, 3)
            each(before, before + jnp.where(s == chunks - 1, per_chunk, 0), second)
            each(lo, hi, first)
            take_point(s, 4)

        each(0, chunks, step_of)
        mp_got[me] = mp_send[me]

        def down(i):
            at = span(i, LANES)
            for n0 in range(0, width, 512):
                dg[at, n0:n0 + 512] = dot(hs[:, at], cot_rows[:, n0:n0 + 512], TN).astype(BF)

        parts = width // CHUNK
        last = order(chunks - 1) * per_chunk
        middle = last + (per_chunk + 1) // 2
        each(0, parts // 2, gate_up)
        each(last, middle, second)
        each(parts // 2, parts * 3 // 4, gate_up)
        each(middle, last + per_chunk, second)
        each(parts * 3 // 4, parts, gate_up)

        each(1, senders, lambda j: part_copy(peer(j), peer(j)).wait_recv())
        mix_all[0] = mp_got[...]

        def t_copy(k):
            return remote(mp_got, mix_all.at[k], t_send.at[k], t_recv.at[k], me, lax.rem(tp + k, seats))

        for k in range(1, seats):
            t_copy(k).start()
        down_parts = hidden // LANES
        each(0, (down_parts + 1) // 2, down)
        for k in range(1, seats):
            t_copy(k).wait()

        slot_mix = jnp.sum(mix_all[...], axis=0)
        grads = []
        for e in range(senders):
            column = to_column(slot_mix[e, 0:1, 0:capacity])
            chosen = pick[e * capacity:(e + 1) * capacity, :].astype(F32)
            grads.append(jnp.sum(column * chosen, axis=0, keepdims=True))
        grads = jnp.concatenate(grads, axis=0)
        mg_first = jnp.sum(jnp.where(is_first, grads, 0.0), axis=0, keepdims=True)
        mg_second = jnp.sum(jnp.where(is_second, grads, 0.0), axis=0, keepdims=True)
        mix_out[0:1, :] = mg_first
        mix_out[1:2, :] = mg_second
        lg_first = mix_first * mix_second * (mg_first - mg_second)
        route_grad = split(jnp.where(is_first, lg_first, jnp.where(is_second, -lg_first, 0.0)))
        raw = dot(route_grad, tok_ref[...])
        norm_scale = 1.0 / math.sqrt(home_rows * senders)
        rt_full[...] = (raw[0:senders] + raw[senders:2 * senders] + raw[2 * senders:]) * norm_scale

        def rt_cols(dest):
            return span((dest * seats + tp) * share // LANES, LANES)

        def r_copy(dest, slot):
            return remote(rt_full.at[:, rt_cols(dest)], rt_got.at[slot], r_send.at[dest], r_recv.at[slot], dest, tp)

        each(1, senders, lambda k: r_copy(peer(k), me).start())
        rt_got[me] = rt_full[:, rt_cols(me)]
        each((down_parts + 1) // 2, down_parts, down)

        def close(items, hops):
            def action(j):
                block = peer(j)
                for array, step in items + [(a, -s) for a, s in hops]:
                    c_copy(array, step, block).wait_send()
                for array, step in hops:
                    y_copy(array, step, block).wait_send()

            return action

        for step in range(1, rows):
            raw_copy(step).wait_send()
        close(mine, [])(0)
        each(1, half, close(near, []))
        each(half, senders, close(far, far_hops))

        def close_back(j):
            block = peer(j)
            for step in range(rows):
                rc_copy(step, block).wait_send()
            for step in range(1, rows):
                ry_copy(step, block).wait_send()

        each(0, senders, close_back)

        def close_dispatch(count):
            def action(k):
                dest = peer(k)
                for i in range(count):
                    ep_copy(i, dest, me).wait_send()
                mix_copy(dest, me).wait_send()

            return action

        each(1, half, close_dispatch(len(near)))
        each(half, senders, close_dispatch(len(far)))

        home[own, :] = terms[own, span(tp, col)]
        each(1, senders, lambda k: home_copy(peer(k), peer(k)).wait_recv())
        cols = router_ref[:, span(tp, col)]
        tg_out[...] = (
            dot(pick[...], home[...], TN) + dot(route_grad, jnp.concatenate([cols, cols, cols], axis=0), TN)
        ).astype(BF)
        each(1, senders, lambda k: r_copy(peer(k), peer(k)).wait_recv())
        rt_out[...] = jnp.sum(rt_got[...], axis=0)

        def close_sends(dest):
            part_copy(dest, me).wait_send()
            home_copy(dest, me).wait_send()
            r_copy(dest, me).wait_send()

        each(1, senders, lambda k: close_sends(peer(k)))

    return body


def layer(tokens, cotangent, routes, router, w_gate, w_up, w_down):
    home_rows, width = tokens.shape
    senders = router.shape[0]
    seats = lax.axis_size("tp")
    rows = seats // 2
    col = width // seats
    hidden = w_gate.shape[1]
    capacity = home_rows * routes.shape[0] * 2 // senders
    slots = senders * capacity
    share = width // (senders * seats)
    vmem = pl.BlockSpec(memory_space=pltpu.VMEM)
    hbm = pl.BlockSpec(memory_space=pltpu.HBM)
    dma = pltpu.SemaphoreType.DMA

    def buf(shape, dtype=BF):
        return pltpu.VMEM(shape, dtype)

    return pl.pallas_call(
        layer_kernel(senders, rows, capacity, col, hidden, share),
        out_shape=(
            buf((home_rows, col)),
            buf((2, home_rows), F32),
            buf((senders, LANES), F32),
            buf((width, hidden)),
            buf((width, hidden)),
            buf((hidden, width)),
        ),
        in_specs=[hbm] * 7,
        out_specs=[vmem] * 6,
        scratch_shapes=[
            buf(tokens.shape), buf(cotangent.shape), buf(routes.shape, routes.dtype), buf(router.shape),
            buf((width, hidden)), buf((width, hidden)), buf((hidden, width)),
            buf((slots, home_rows)), buf((rows, slots, col)), buf((slots, col)),
            buf((rows - 1, home_rows, col)), buf((rows - 1, slots // 2, col)),
            buf((senders, senders, LANES), F32), buf((senders, senders, LANES), F32),
            buf((slots, width)), buf((slots, width)),
            buf((slots, hidden)), buf((slots, hidden)), buf((slots, hidden)), buf((slots, width)),
            buf((senders, 8, LANES), F32), buf((senders, 8, LANES), F32), buf((seats, senders, 8, LANES), F32),
            buf((rows, slots, col)), buf((rows - 1, slots, col)), buf((slots, col)),
            buf((senders, width), F32), buf((senders, senders, LANES), F32),
            dma((7,)), dma((rows,)), dma((rows,)),
            dma((2 * rows, senders)), dma((2 * rows, senders)),
            dma((2, rows, senders)), dma((2, rows, senders)),
            dma((2, 2 * rows, senders)), dma((2, 2 * rows, senders)),
            dma((senders,)), dma((senders,)),
            dma((rows, senders)), dma((rows, senders)),
            dma((rows, senders)), dma((rows, senders)),
            dma((senders,)), dma((senders,)),
            dma((senders,)), dma((senders,)),
            dma((seats,)), dma((seats,)),
            dma((senders,)), dma((senders,)),
        ],
        compiler_params=pltpu.CompilerParams(has_side_effects=True, collective_id=0, vmem_limit_bytes=46 << 20),
        name="layer",
    )(tokens, cotangent, routes, router, w_gate, w_up, w_down)


def output_kernel(share):
    def body(tg, mix, rt, gg, ug, dg, tg_out, mix_out, rt_out, gg_out, ug_out, dg_out, sem):
        copies = [pltpu.make_async_copy(src, dst, sem.at[i])
                  for i, (src, dst) in enumerate(((gg, gg_out), (ug, ug_out), (dg, dg_out), (tg, tg_out), (mix, mix_out)))]
        for copy in copies:
            copy.start()
        offset = (lax.axis_index("ep") * lax.axis_size("tp") + lax.axis_index("tp")) * share % LANES
        total = jnp.zeros(rt_out.shape, F32)
        for start in range(0, LANES, share):
            total = total + jnp.where(offset == start, rt[:, start:start + share], 0.0)
        rt_out[...] = total
        for copy in copies:
            copy.wait()

    return body


def outputs(token_grad, mixing, router_rows, gate_grad, up_grad, down_grad, share):
    vmem = pl.BlockSpec(memory_space=pltpu.VMEM)
    hbm = pl.BlockSpec(memory_space=pl.ANY)
    like = [jax.ShapeDtypeStruct(x.shape, x.dtype) for x in (token_grad, mixing, router_rows, gate_grad, up_grad, down_grad)]
    like[2] = jax.ShapeDtypeStruct((router_rows.shape[0], share), F32)
    return pl.pallas_call(
        output_kernel(share),
        out_shape=like,
        in_specs=[vmem] * 6,
        out_specs=[hbm, hbm, vmem, hbm, hbm, hbm],
        scratch_shapes=[pltpu.SemaphoreType.DMA((5,))],
        compiler_params=pltpu.CompilerParams(vmem_limit_bytes=4 << 20),
        name="outputs",
    )(token_grad, mixing, router_rows, gate_grad, up_grad, down_grad)


def local(tokens, routes, router_matrix, cotangent, gate_proj, up_proj, down_proj):
    share = tokens.shape[1] // (lax.axis_size("ep") * lax.axis_size("tp"))
    results = layer(
        tokens, cotangent, routes.T, router_matrix.T, gate_proj[0], up_proj[0], down_proj[0]
    )
    token_grad, mixing, router_grad, gate_grad, up_grad, down_grad = outputs(*results, share)
    return (token_grad, mixing.T, router_grad.T, gate_grad[None], up_grad[None], down_grad[None])


def solution(mesh):
    return jax.shard_map(
        local,
        mesh=mesh,
        in_specs=(
            P("ep", None),
            P("ep", None),
            P(),
            P("ep", "tp"),
            P("ep", None, "tp"),
            P("ep", None, "tp"),
            P("ep", "tp", None),
        ),
        out_specs=(
            P("ep", "tp"),
            P("ep", None),
            P(("ep", "tp"), None),
            P("ep", None, "tp"),
            P("ep", None, "tp"),
            P("ep", "tp", None),
        ),
        check_vma=False,
    )
```

```python
import math

import jax
import jax.numpy as jnp
from jax import lax
from jax.experimental import pallas as pl
from jax.experimental.pallas import tpu as pltpu
from jax.sharding import PartitionSpec as P

MESH = pl.DeviceIdType.MESH
LANES = 128
CHUNK = 256
OUTER_TAKES = (4, 6, 6, 6, 6, 7, 8, 8, 8, 8, 8, 8, 8)
INNER_TAKES = (4, 6, 6, 6, 6, 6, 8, 8, 8, 8, 8, 8, 8)
BF = jnp.bfloat16
F32 = jnp.float32
NN = (((1,), (0,)), ((), ()))
NT = (((1,), (1,)), ((), ()))
TN = (((0,), (0,)), ((), ()))


def dot(a, b, dims=NN):
    return lax.dot_general(a, b, dims, preferred_element_type=F32)


def remote(src, dst, send, recv, ep, tp):
    return pltpu.make_async_remote_copy(
        src_ref=src,
        dst_ref=dst,
        send_sem=send,
        recv_sem=recv,
        device_id=(ep, tp),
        device_id_type=MESH,
    )


def pair(me, k, size):
    return sum((me // bit + k // bit) % 2 * bit for bit in (1 << b for b in range(size.bit_length() - 1)))


def span(start, size):
    return pl.ds(pl.multiple_of(start * size, size), size)


def each(lo, hi, action):
    def step(k, carry):
        action(k)
        return carry

    lax.fori_loop(lo, hi, step, 0)


def split(value):
    high = value.astype(BF)
    rest = value - high.astype(F32)
    middle = rest.astype(BF)
    low = (rest - middle.astype(F32)).astype(BF)
    return jnp.concatenate([high, middle, low], axis=0)


def layer_kernel(senders, rows, capacity, col, hidden, share):
    seats = 2 * rows
    width = col * seats
    per_chunk = max(1, min(senders, CHUNK // capacity))
    chunk = per_chunk * capacity
    chunks = senders // per_chunk
    half = max(senders // 2, 1)

    def body(tok_hbm, cot_hbm, routes_hbm, router_hbm, wg_hbm, wu_hbm, wd_hbm,
             tg_out, mix_out, rt_out, gg, ug, dg,
             tok_ref, cot_ref, routes_ref, router_ref, wg, wu, wd, pick, tok_send, cot_send, cot_raw, cot_more, mix_send, mix_in, tok_rows, cot_rows,
             hs, gb, ub, terms, mp_send, mp_got, mix_all, c_buf, y_buf, home, rt_full, rt_got,
             w_sem, raw_send, raw_recv, ep_send, ep_recv, y_send, y_recv, c_send, c_recv, m_send, m_recv,
             rc_send, rc_recv, ry_send, ry_recv, h_send, h_recv, p_send, p_recv, t_send, t_recv, r_send, r_recv):
        me = lax.axis_index("ep")
        tp = lax.axis_index("tp")
        row = tp // 2
        core = tp % 2
        partner = row * 2 + (1 - core)
        my_chunk = me // per_chunk

        def seat(step, side):
            return lax.rem(row + step + rows, rows) * 2 + side

        def peer(k):
            return pair(me, k, senders)

        def raw_copy(step):
            return remote(cot_ref, cot_raw.at[step - 1], raw_send.at[step - 1], raw_recv.at[step - 1], me, seat(step, core))

        barrier = pltpu.get_barrier_semaphore()
        each(1, senders, lambda k: pl.semaphore_signal(barrier, inc=1, device_id=(peer(k), tp), device_id_type=MESH))
        for k in range(1, seats):
            pl.semaphore_signal(barrier, inc=1, device_id=(me, lax.rem(tp + k, seats)), device_id_type=MESH)

        loads = [pltpu.make_async_copy(src, dst, w_sem.at[i])
                 for i, (src, dst) in enumerate((
                     (routes_hbm, routes_ref), (tok_hbm, tok_ref), (router_hbm, router_ref), (cot_hbm, cot_ref),
                     (wg_hbm, wg), (wu_hbm, wu), (wd_hbm, wd)))]
        for load in loads:
            load.start()
        loads[0].wait()
        loads[3].wait()

        ids = lax.broadcasted_iota(jnp.int32, (senders, tok_ref.shape[0]), 0)
        is_first = ids == routes_ref[0:1, :]
        is_second = ids == routes_ref[1:2, :]
        member = jnp.where(is_first | is_second, 1.0, 0.0)
        home_rows = tok_ref.shape[0]
        earlier = lax.broadcasted_iota(jnp.int32, (home_rows, home_rows), 0) < lax.broadcasted_iota(
            jnp.int32, (home_rows, home_rows), 1)
        rank = dot(member.astype(BF), jnp.where(earlier, 1.0, 0.0).astype(BF))
        place = jnp.where(member > 0.0, rank, -1.0)
        slot_ids = lax.broadcasted_iota(jnp.int32, (capacity, home_rows), 0).astype(F32)
        for e in range(senders):
            pick[e * capacity:(e + 1) * capacity, :] = jnp.where(slot_ids == place[e:e + 1, :], 1.0, 0.0).astype(BF)

        loads[1].wait()

        cot_send[...] = dot(pick[...], cot_ref[...]).astype(BF)
        for r in range(rows):
            tok_send[r] = dot(pick[...], tok_ref[:, span(seat(r, core), col)]).astype(BF)
        pl.semaphore_wait(barrier, senders - 1 + seats - 1)
        for step in range(1, rows):
            raw_copy(step).start()
        own = span(me, capacity)
        tok_rows[own, :] = dot(pick[own, :], tok_ref[...]).astype(BF)
        cot_rows[own, span(tp, col)] = cot_send[own, :]

        arrays = (tok_rows, cot_rows)

        def piece(array, block, tp_col):
            return array.at[span(block, capacity), span(tp_col, col)]

        mine = [(1, -j) for j in range(rows)]
        far = [(1, 0), (0, 0)]
        near = far + [(0, j) for j in range(1, rows)]
        close = near + [(1, -j) for j in range(1, rows)]
        far_hops = [(a, j) for j in range(1, rows) for a in (1, 0)]
        near_hops = [(1, j) for j in range(1, rows)]
        close_first = my_chunk * per_chunk

        def ep_copy(i, dest, block):
            array, which = close[i]
            if array == 1 and which < 0:
                source = cot_more.at[-which - 1, span(dest - close_first, capacity), :]
            else:
                source = (tok_send.at[which] if array == 0 else cot_send).at[span(dest, capacity), :]
            return remote(source, piece(arrays[array], block, seat(which, core)),
                          ep_send.at[dest], ep_recv.at[min(i, 1), block], dest, tp)

        def bulk(block, count, send, recv):
            at = tok_rows.at[span(block, capacity), pl.ds(0, count * col)]
            return remote(at, at, send, recv, me, partner)

        def mix_copy(dest, block):
            return remote(mix_send.at[dest], mix_in.at[block], m_send.at[0], m_recv.at[block], dest, tp)

        def y_copy(array, step, block):
            at = piece(arrays[array], block, tp)
            return remote(at, at, y_send.at[block], y_recv.at[array, step - 1, block], me, seat(step, core))

        def y_arrival(array, step, block):
            at = piece(arrays[array], block, seat(-step, core))
            return remote(at, at, y_send.at[block], y_recv.at[array, step - 1, block], me, seat(step, core))

        def c_copy(array, step, block):
            at = piece(arrays[array], block, seat(step, core))
            return remote(at, at, c_send.at[block], c_recv.at[block], me, partner)

        inner = (my_chunk + my_chunk // 2) % 2

        def choose(s, values):
            return sum(jnp.where(s == i, v, 0) for i, v in enumerate(values))

        def order(s):
            if chunks != 4:
                return s
            return jnp.where(inner == 1, choose(s, (0, 1, 2, 3)), choose(s, (0, 2, 1, 3)))

        def take_order(s):
            if chunks != 4:
                return s
            return jnp.where(inner == 1, s, choose(s, (2, 0, 1, 3)))

        def send(lo, hi):
            def action(k):
                for i in range(lo, hi):
                    ep_copy(i, peer(k), me).start()

            return action

        def send_far(on):
            for s in range(half // per_chunk, chunks):
                start = s * per_chunk
                each(start, start + per_chunk * on, send(0, len(far)))

        c_copy(1, 0, me).start()
        each(1, half, send(0, len(near)))
        loads[2].wait()
        logits = dot(router_ref[...], tok_ref[...], NT)
        chosen_first = jnp.sum(jnp.where(is_first, logits, 0.0), axis=0, keepdims=True)
        chosen_second = jnp.sum(jnp.where(is_second, logits, 0.0), axis=0, keepdims=True)
        mix_first = 1.0 / (1.0 + jnp.exp(chosen_second - chosen_first))
        mix_second = 1.0 / (1.0 + jnp.exp(chosen_first - chosen_second))
        mix_value = jnp.where(is_first, mix_first, jnp.where(is_second, mix_second, 0.0)).astype(BF)
        for e in range(senders):
            mix_send[e, :, 0:capacity] = dot(mix_value, pick[e * capacity:(e + 1) * capacity, :], NT)
        mix_in[me] = mix_send[me]
        each(1, senders, lambda k: mix_copy(peer(k), me).start())
        send_far(inner)
        for step in range(1, rows):
            raw_copy(step).wait_recv()
            cot_more[step - 1] = dot(pick[span(my_chunk, chunk), :], cot_raw[step - 1]).astype(BF)
            cot_rows[own, span(seat(-step, core), col)] = cot_more[step - 1, span(me - close_first, capacity), :]
            c_copy(1, -step, me).start()
        each(1, per_chunk, send(len(near), len(close)))
        send_far(1 - inner)

        def take(items, hops):
            def action(j):
                block = peer(j)
                for i, (array, step) in enumerate(items):
                    if i == 0:
                        ep_copy(0, block, block).wait_recv()
                    if i == 1:
                        bulk(block, len(items) - 1, ep_send.at[block], ep_recv.at[1, block]).wait_recv()
                    for a, hop in hops:
                        if a == array and step == 0:
                            y_copy(array, hop, block).start()
                    c_copy(array, step, block).start()

            return action

        def pass_on(hops):
            def action(j):
                block = peer(j)
                for array, step in hops:
                    y_arrival(array, step, block).wait_recv()
                    c_copy(array, -step, block).start()

            return action

        def settle(items, hops):
            def action(j):
                block = peer(j)
                bulk(block, len(items) + len(hops), c_send.at[block], c_recv.at[block]).wait_recv()

            return action

        def arrive_mix(j):
            mix_copy(peer(j), peer(j)).wait_recv()

        def home_copy(dest, slot):
            return remote(piece(terms, dest, tp), home.at[span(slot, capacity), :],
                          h_send.at[0], h_recv.at[0], dest, tp)

        def part_copy(dest, slot):
            return remote(mp_send.at[dest], mp_got.at[slot], p_send.at[0], p_recv.at[0], dest, tp)

        def rc_copy(step, block):
            return remote(piece(terms, block, seat(step, 1 - core)), c_buf.at[step, span(block, capacity), :],
                          rc_send.at[block], rc_recv.at[step, block], me, partner)

        def ry_copy(step, block):
            return remote(piece(terms, block, seat(step, core)), y_buf.at[step - 1, span(block, capacity), :],
                          ry_send.at[block], ry_recv.at[step - 1, block], me, seat(step, core))

        def first(j):
            block = peer(j)
            at = span(block, capacity)
            for step in range(1, rows):
                rc_copy(step, block).wait_recv()
                cols = span(seat(step, core), col)
                terms[at, cols] = (terms[at, cols].astype(F32) + c_buf[step, at, :].astype(F32)).astype(BF)
                ry_copy(step, block).start()

        def second(j):
            block = peer(j)
            at = span(block, capacity)
            rc_copy(0, block).wait_recv()
            value = terms[at, span(tp, col)].astype(F32) + c_buf[0, at, :].astype(F32)
            for step in range(1, rows):
                ry_copy(step, block).wait_recv()
                value = value + y_buf[step - 1, at, :].astype(F32)
            terms[at, span(tp, col)] = value.astype(BF)

            @pl.when(j > 0)
            def _():
                home_copy(block, me).start()

        diagonal = lax.broadcasted_iota(jnp.int32, (capacity, capacity), 0) == lax.broadcasted_iota(
            jnp.int32, (capacity, capacity), 1)

        def to_column(values):
            return jnp.sum(jnp.where(diagonal, values, 0.0), axis=1, keepdims=True)

        def to_row(values):
            return jnp.sum(jnp.where(diagonal, values, 0.0), axis=0, keepdims=True)

        def forward(which):
            at = span(which, chunk)
            mixes = jnp.concatenate(
                [to_column(mix_in[which * per_chunk + i, pl.ds(me, 1), :][:, 0:capacity]) for i in range(per_chunk)],
                axis=0)
            x = tok_rows[at, :]
            dy = cot_rows[at, :]
            total = jnp.zeros((chunk, 1), F32)
            for n0 in range(0, hidden, CHUNK):
                n = min(CHUNK, hidden - n0)
                gate = dot(x, wg[:, n0:n0 + n])
                up = dot(x, wu[:, n0:n0 + n])
                back = dot(dy, wd[n0:n0 + n, :], NT)
                sig = 1.0 / (1.0 + jnp.exp(-gate))
                active = gate * sig
                inner = active * up
                total = total + jnp.sum(inner * back, axis=1, keepdims=True)
                scaled = mixes * back
                gb[at, n0:n0 + n] = (scaled * up * sig * (1.0 + gate * (1.0 - sig))).astype(BF)
                ub[at, n0:n0 + n] = (scaled * active).astype(BF)
                hs[at, n0:n0 + n] = (mixes * inner).astype(BF)
            for i in range(per_chunk):
                line = to_row(total[i * capacity:(i + 1) * capacity, :])
                mp_send[which * per_chunk + i, :, 0:capacity] = jnp.broadcast_to(line, (8, capacity))

        def backward(which, lo):
            at = span(which, chunk)
            gate_back = gb[at, :]
            up_back = ub[at, :]
            for step in list(range(1, rows)) + [0]:
                for side in (1 - core, core):
                    cols = span(seat(step, side), col)
                    terms[at, cols] = (dot(gate_back, wg[cols, :], NT) + dot(up_back, wu[cols, :], NT)).astype(BF)
                for i in range(per_chunk):
                    rc_copy(step, peer(lo + i)).start()

        def ranged(own_action, close_action, near_action, far_action):
            def run(lo, hi):
                if own_action is not None:
                    each(lo, jnp.minimum(hi, 1), own_action)
                if close_action is not None:
                    each(jnp.maximum(lo, 1), jnp.minimum(hi, per_chunk), close_action)
                each(jnp.maximum(lo, per_chunk), jnp.minimum(hi, half), near_action)
                each(jnp.maximum(lo, half), hi, far_action)

            return run

        take_range = ranged(None, take(close, []), take(near, near_hops), take(far, far_hops))
        pass_range = ranged(None, None, pass_on(near_hops), pass_on(far_hops))
        settle_range = ranged(settle(mine, []), settle(close, []), settle(near, near_hops), settle(far, far_hops))
        part = (per_chunk + 1) // 2

        def take_halves(lo, hi):
            def one(h):
                start = take_order(h // 2) * per_chunk + h % 2 * part
                take_range(start, start + part)

            each(lo, hi, one)

        def taken(s, point):
            def of(table):
                return choose(s, [table[3 * i + point] for i in range(4)])

            return jnp.where(inner == 1, of(INNER_TAKES), of(OUTER_TAKES))

        def take_point(s, point):
            take_halves(taken(s, point - 1), taken(s, point))

        take_halves(0, 4)

        def joined(ref, steps, cols):
            return jnp.concatenate([ref[span(pair(my_chunk, order(s), chunks), chunk), cols] for s in steps], axis=0)

        first_half, second_half = range(chunks // 2), range(chunks // 2, chunks)

        def down_early(i):
            at = span(i, LANES)
            x = joined(hs, range(chunks - 1), at)
            for n0 in range(0, width, 512):
                dg[at, n0:n0 + 512] = dot(x, joined(cot_rows, range(chunks - 1), slice(n0, n0 + 512)), TN).astype(BF)

        def down(i):
            at = span(i, LANES)
            x = joined(hs, [chunks - 1], at)
            for n0 in range(0, width, 512):
                more = dot(x, joined(cot_rows, [chunks - 1], slice(n0, n0 + 512)), TN)
                dg[at, n0:n0 + 512] = (dg[at, n0:n0 + 512].astype(F32) + more).astype(BF)

        def gate_up_early(i):
            at = span(i, CHUNK)
            x = joined(tok_rows, first_half, at)
            gg[at, :] = dot(x, joined(gb, first_half, slice(None)), TN).astype(BF)
            ug[at, :] = dot(x, joined(ub, first_half, slice(None)), TN).astype(BF)

        def gate_up(i):
            at = span(i, CHUNK)
            x = joined(tok_rows, second_half, at)
            gg[at, :] = (gg[at, :].astype(F32) + dot(x, joined(gb, second_half, slice(None)), TN)).astype(BF)
            ug[at, :] = (ug[at, :].astype(F32) + dot(x, joined(ub, second_half, slice(None)), TN)).astype(BF)

        def step_of(s):
            lo = order(s) * per_chunk
            hi = lo + per_chunk
            before = order(jnp.maximum(s - 1, 0)) * per_chunk
            earlier_chunk = order(jnp.maximum(s - 2, 0)) * per_chunk
            which = pair(my_chunk, order(s), chunks)

            each(0, jnp.where(s == chunks - 1, hidden // LANES, 0), down_early)
            pass_range(lo, hi)
            settle_range(lo, hi)
            each(jnp.maximum(lo, 1), hi, arrive_mix)

            @pl.when(s == 0)
            def _():
                for load in loads[4:]:
                    load.wait()

            forward(which)
            each(jnp.maximum(lo, 1), hi, lambda j: part_copy(peer(j), me).start())
            take_point(s, 1)
            each(earlier_chunk, earlier_chunk + jnp.where(s == 2, per_chunk, 0), second)
            each(before, before + jnp.where(s > 1, per_chunk, 0), second)
            backward(which, lo)
            each(lo, hi, first)
            take_point(s, 2)
            each(0, jnp.where(s == chunks // 2 - 1, width // CHUNK, 0), gate_up_early)
            take_point(s, 3)

        each(0, chunks, step_of)
        mp_got[me] = mp_send[me]

        parts = width // CHUNK
        last = order(chunks - 1) * per_chunk
        middle = last + (per_chunk + 1) // 2
        each(0, parts // 2, gate_up)
        others = pl.ds(0, senders - 1)

        def all_parts():
            return remote(mp_send.at[others], mp_got.at[others], p_send.at[0], p_recv.at[0], me, partner)

        all_parts().wait_recv()
        mix_all[0] = mp_got[...]

        def t_copy(k):
            return remote(mp_got, mix_all.at[k], t_send.at[k], t_recv.at[k], me, lax.rem(tp + k, seats))

        for k in range(1, seats):
            t_copy(k).start()
        each(last, middle, second)
        each(parts // 2, parts * 3 // 4, gate_up)
        for k in range(1, seats):
            t_copy(k).wait()

        slot_mix = jnp.sum(mix_all[...], axis=0)
        grads = []
        for e in range(senders):
            column = to_column(slot_mix[e, 0:1, 0:capacity])
            chosen = pick[e * capacity:(e + 1) * capacity, :].astype(F32)
            grads.append(jnp.sum(column * chosen, axis=0, keepdims=True))
        grads = jnp.concatenate(grads, axis=0)
        mg_first = jnp.sum(jnp.where(is_first, grads, 0.0), axis=0, keepdims=True)
        mg_second = jnp.sum(jnp.where(is_second, grads, 0.0), axis=0, keepdims=True)
        mix_out[0:1, :] = mg_first
        mix_out[1:2, :] = mg_second
        lg_first = mix_first * mix_second * (mg_first - mg_second)
        route_grad = split(jnp.where(is_first, lg_first, jnp.where(is_second, -lg_first, 0.0)))
        raw = dot(route_grad, tok_ref[...])
        norm_scale = 1.0 / math.sqrt(home_rows * senders)
        rt_full[...] = (raw[0:senders] + raw[senders:2 * senders] + raw[2 * senders:]) * norm_scale

        def rt_cols(dest):
            return span((dest * seats + tp) * share // LANES, LANES)

        def r_copy(dest, slot):
            return remote(rt_full.at[:, rt_cols(dest)], rt_got.at[slot], r_send.at[0], r_recv.at[0], dest, tp)

        each(1, senders, lambda k: r_copy(peer(k), me).start())
        rt_got[me] = rt_full[:, rt_cols(me)]
        each(middle, last + per_chunk, second)
        each(parts * 3 // 4, parts, gate_up)
        each(0, hidden // LANES, down)

        def finish(items, hops):
            def action(j):
                block = peer(j)
                bulk(block, len(items) + len(hops), c_send.at[block], c_recv.at[block]).wait_send()
                if hops:
                    bulk(block, len(hops), y_send.at[block], y_recv.at[0, 0, block]).wait_send()
                if items is not mine:
                    bulk(block, len(items), ep_send.at[block], ep_recv.at[0, block]).wait_send()

            return action

        for step in range(1, rows):
            raw_copy(step).wait_send()
        finish(mine, [])(0)
        each(1, per_chunk, finish(close, []))
        each(per_chunk, half, finish(near, near_hops))
        each(half, senders, finish(far, far_hops))

        def close_back(j):
            block = peer(j)
            bulk(block, rows, rc_send.at[block], rc_recv.at[0, block]).wait_send()
            bulk(block, rows - 1, ry_send.at[block], ry_recv.at[0, block]).wait_send()

        each(0, senders, close_back)
        remote(mix_send.at[others], mix_in.at[others], m_send.at[0], m_recv.at[0], me, partner).wait_send()
        all_parts().wait_send()

        def all_home():
            at = home.at[pl.ds(0, (senders - 1) * capacity), :]
            return remote(at, at, h_send.at[0], h_recv.at[0], me, partner)

        def all_router():
            at = rt_got.at[others]
            return remote(at, at, r_send.at[0], r_recv.at[0], me, partner)

        home[own, :] = terms[own, span(tp, col)]
        all_home().wait_recv()
        cols = router_ref[:, span(tp, col)]
        tg_out[...] = (
            dot(pick[...], home[...], TN) + dot(route_grad, jnp.concatenate([cols, cols, cols], axis=0), TN)
        ).astype(BF)
        all_router().wait_recv()
        rt_out[...] = jnp.sum(rt_got[...], axis=0)
        all_home().wait_send()
        all_router().wait_send()

    return body


def layer(tokens, cotangent, routes, router, w_gate, w_up, w_down):
    home_rows, width = tokens.shape
    senders = router.shape[0]
    seats = lax.axis_size("tp")
    rows = seats // 2
    col = width // seats
    hidden = w_gate.shape[1]
    capacity = home_rows * routes.shape[0] * 2 // senders
    slots = senders * capacity
    share = width // (senders * seats)
    vmem = pl.BlockSpec(memory_space=pltpu.VMEM)
    hbm = pl.BlockSpec(memory_space=pltpu.HBM)
    dma = pltpu.SemaphoreType.DMA

    def buf(shape, dtype=BF):
        return pltpu.VMEM(shape, dtype)

    return pl.pallas_call(
        layer_kernel(senders, rows, capacity, col, hidden, share),
        out_shape=(
            buf((home_rows, col)),
            buf((2, home_rows), F32),
            buf((senders, LANES), F32),
            buf((width, hidden)),
            buf((width, hidden)),
            buf((hidden, width)),
        ),
        in_specs=[hbm] * 7,
        out_specs=[vmem] * 6,
        scratch_shapes=[
            buf(tokens.shape), buf(cotangent.shape), buf(routes.shape, routes.dtype), buf(router.shape),
            buf((width, hidden)), buf((width, hidden)), buf((hidden, width)),
            buf((slots, home_rows)), buf((rows, slots, col)), buf((slots, col)),
            buf((rows - 1, home_rows, col)), buf((rows - 1, max(CHUNK, capacity), col)),
            buf((senders, senders, LANES), F32), buf((senders, senders, LANES), F32),
            buf((slots, width)), buf((slots, width)),
            buf((slots, hidden)), buf((slots, hidden)), buf((slots, hidden)), buf((slots, width)),
            buf((senders, 8, LANES), F32), buf((senders, 8, LANES), F32), buf((seats, senders, 8, LANES), F32),
            buf((rows, slots, col)), buf((rows - 1, slots, col)), buf((slots, col)),
            buf((senders, width), F32), buf((senders, senders, LANES), F32),
            dma((7,)), dma((rows - 1,)), dma((rows - 1,)),
            dma((senders,)), dma((2, senders)),
            dma((senders,)), dma((2, rows - 1, senders)),
            dma((senders,)), dma((senders,)),
            dma((1,)), dma((senders,)),
            dma((senders,)), dma((rows, senders)),
            dma((senders,)), dma((rows - 1, senders)),
            dma((1,)), dma((1,)),
            dma((1,)), dma((1,)),
            dma((seats,)), dma((seats,)),
            dma((1,)), dma((1,)),
        ],
        compiler_params=pltpu.CompilerParams(has_side_effects=True, collective_id=0, vmem_limit_bytes=46 << 20),
        name="layer",
    )(tokens, cotangent, routes, router, w_gate, w_up, w_down)


def output_kernel(share):
    def body(tg, mix, rt, gg, ug, dg, tg_out, mix_out, rt_out, gg_out, ug_out, dg_out, sem):
        copies = [pltpu.make_async_copy(src, dst, sem.at[i])
                  for i, (src, dst) in enumerate(((gg, gg_out), (ug, ug_out), (dg, dg_out), (tg, tg_out), (mix, mix_out)))]
        for copy in copies:
            copy.start()
        offset = (lax.axis_index("ep") * lax.axis_size("tp") + lax.axis_index("tp")) * share % LANES
        total = jnp.zeros(rt_out.shape, F32)
        for start in range(0, LANES, share):
            total = total + jnp.where(offset == start, rt[:, start:start + share], 0.0)
        rt_out[...] = total
        for copy in copies:
            copy.wait()

    return body


def outputs(token_grad, mixing, router_rows, gate_grad, up_grad, down_grad, share):
    vmem = pl.BlockSpec(memory_space=pltpu.VMEM)
    hbm = pl.BlockSpec(memory_space=pl.ANY)
    like = [jax.ShapeDtypeStruct(x.shape, x.dtype) for x in (token_grad, mixing, router_rows, gate_grad, up_grad, down_grad)]
    like[2] = jax.ShapeDtypeStruct((router_rows.shape[0], share), F32)
    return pl.pallas_call(
        output_kernel(share),
        out_shape=like,
        in_specs=[vmem] * 6,
        out_specs=[hbm, hbm, vmem, hbm, hbm, hbm],
        scratch_shapes=[pltpu.SemaphoreType.DMA((5,))],
        compiler_params=pltpu.CompilerParams(vmem_limit_bytes=4 << 20),
        name="outputs",
    )(token_grad, mixing, router_rows, gate_grad, up_grad, down_grad)


def local(tokens, routes, router_matrix, cotangent, gate_proj, up_proj, down_proj):
    share = tokens.shape[1] // (lax.axis_size("ep") * lax.axis_size("tp"))
    results = layer(
        tokens, cotangent, routes.T, router_matrix.T, gate_proj[0], up_proj[0], down_proj[0]
    )
    token_grad, mixing, router_grad, gate_grad, up_grad, down_grad = outputs(*results, share)
    return (token_grad, mixing.T, router_grad.T, gate_grad[None], up_grad[None], down_grad[None])


def solution(mesh):
    return jax.shard_map(
        local,
        mesh=mesh,
        in_specs=(
            P("ep", None),
            P("ep", None),
            P(),
            P("ep", "tp"),
            P("ep", None, "tp"),
            P("ep", None, "tp"),
            P("ep", "tp", None),
        ),
        out_specs=(
            P("ep", "tp"),
            P("ep", None),
            P(("ep", "tp"), None),
            P("ep", None, "tp"),
            P("ep", None, "tp"),
            P("ep", "tp", None),
        ),
        check_vma=False,
    )
```

```python
import math

import jax
import jax.numpy as jnp
from jax import lax
from jax.experimental import pallas as pl
from jax.experimental.pallas import tpu as pltpu
from jax.sharding import PartitionSpec as P

MESH = pl.DeviceIdType.MESH
LANES = 128
CHUNK = 256
OUTER_TAKES = (4, 4, 6, 6, 6, 7, 8, 8, 8, 8, 8, 8, 8)
INNER_TAKES = (4, 6, 6, 6, 6, 6, 8, 8, 8, 8, 8, 8, 8)
BF = jnp.bfloat16
F32 = jnp.float32
NN = (((1,), (0,)), ((), ()))
NT = (((1,), (1,)), ((), ()))
TN = (((0,), (0,)), ((), ()))


def dot(a, b, dims=NN):
    return lax.dot_general(a, b, dims, preferred_element_type=F32)


def remote(src, dst, send, recv, ep, tp):
    return pltpu.make_async_remote_copy(
        src_ref=src,
        dst_ref=dst,
        send_sem=send,
        recv_sem=recv,
        device_id=(ep, tp),
        device_id_type=MESH,
    )


def pair(me, k, size):
    return sum((me // bit + k // bit) % 2 * bit for bit in (1 << b for b in range(size.bit_length() - 1)))


def span(start, size):
    return pl.ds(pl.multiple_of(start * size, size), size)


def each(lo, hi, action):
    def step(k, carry):
        action(k)
        return carry

    lax.fori_loop(lo, hi, step, 0)


def split(value):
    high = value.astype(BF)
    rest = value - high.astype(F32)
    middle = rest.astype(BF)
    low = (rest - middle.astype(F32)).astype(BF)
    return jnp.concatenate([high, middle, low], axis=0)


def layer_kernel(senders, rows, capacity, col, hidden, share):
    seats = 2 * rows
    width = col * seats
    per_chunk = max(1, min(senders, CHUNK // capacity))
    chunk = per_chunk * capacity
    chunks = senders // per_chunk
    half = max(senders // 2, 1)

    def body(tok_hbm, cot_hbm, routes_hbm, router_hbm, wg_hbm, wu_hbm, wd_hbm,
             tg_out, mix_out, rt_out, gg, ug, dg,
             tok_ref, cot_ref, routes_ref, router_ref, wg, wu, wd, pick, tok_send, cot_send, cot_raw, cot_more, mix_send, mix_in, tok_rows, cot_rows,
             hs, gb, ub, terms, mp_send, mp_got, mix_all, c_buf, y_buf, home, rt_full, rt_got,
             w_sem, raw_send, raw_recv, ep_send, ep_recv, y_send, y_recv, c_send, c_recv, m_send, m_recv,
             rc_send, rc_recv, ry_send, ry_recv, h_send, h_recv, p_send, p_recv, t_send, t_recv, r_send, r_recv):
        me = lax.axis_index("ep")
        tp = lax.axis_index("tp")
        row = tp // 2
        core = tp % 2
        partner = row * 2 + (1 - core)
        my_chunk = me // per_chunk

        def seat(step, side):
            return lax.rem(row + step + rows, rows) * 2 + side

        def peer(k):
            return pair(me, k, senders)

        def raw_copy(step):
            return remote(cot_ref, cot_raw.at[step - 1], raw_send.at[step - 1], raw_recv.at[step - 1], me, seat(step, core))

        barrier = pltpu.get_barrier_semaphore()
        each(1, senders, lambda k: pl.semaphore_signal(barrier, inc=1, device_id=(peer(k), tp), device_id_type=MESH))
        for k in range(1, seats):
            pl.semaphore_signal(barrier, inc=1, device_id=(me, lax.rem(tp + k, seats)), device_id_type=MESH)

        loads = [pltpu.make_async_copy(src, dst, w_sem.at[i])
                 for i, (src, dst) in enumerate((
                     (routes_hbm, routes_ref), (tok_hbm, tok_ref), (router_hbm, router_ref), (cot_hbm, cot_ref),
                     (wg_hbm, wg), (wu_hbm, wu), (wd_hbm, wd)))]
        for load in loads:
            load.start()
        loads[0].wait()
        loads[3].wait()

        ids = lax.broadcasted_iota(jnp.int32, (senders, tok_ref.shape[0]), 0)
        is_first = ids == routes_ref[0:1, :]
        is_second = ids == routes_ref[1:2, :]
        member = jnp.where(is_first | is_second, 1.0, 0.0)
        home_rows = tok_ref.shape[0]
        earlier = lax.broadcasted_iota(jnp.int32, (home_rows, home_rows), 0) < lax.broadcasted_iota(
            jnp.int32, (home_rows, home_rows), 1)
        rank = dot(member.astype(BF), jnp.where(earlier, 1.0, 0.0).astype(BF))
        place = jnp.where(member > 0.0, rank, -1.0)
        slot_ids = lax.broadcasted_iota(jnp.int32, (capacity, home_rows), 0).astype(F32)
        for e in range(senders):
            pick[e * capacity:(e + 1) * capacity, :] = jnp.where(slot_ids == place[e:e + 1, :], 1.0, 0.0).astype(BF)

        loads[1].wait()

        cot_send[...] = dot(pick[...], cot_ref[...]).astype(BF)
        for r in range(rows):
            tok_send[r] = dot(pick[...], tok_ref[:, span(seat(r, core), col)]).astype(BF)
        pl.semaphore_wait(barrier, senders - 1 + seats - 1)
        for step in range(1, rows):
            raw_copy(step).start()
        own = span(me, capacity)
        tok_rows[own, :] = dot(pick[own, :], tok_ref[...]).astype(BF)
        cot_rows[own, span(tp, col)] = cot_send[own, :]

        arrays = (tok_rows, cot_rows)

        def piece(array, block, tp_col):
            return array.at[span(block, capacity), span(tp_col, col)]

        mine = [(1, -j) for j in range(rows)]
        far = [(1, 0), (0, 0)]
        near = far + [(0, j) for j in range(1, rows)]
        close = near + [(1, -j) for j in range(1, rows)]
        far_hops = [(a, j) for j in range(1, rows) for a in (1, 0)]
        near_hops = [(1, j) for j in range(1, rows)]
        close_first = my_chunk * per_chunk

        def ep_copy(i, dest, block):
            array, which = close[i]
            if array == 1 and which < 0:
                source = cot_more.at[-which - 1, span(dest - close_first, capacity), :]
            else:
                source = (tok_send.at[which] if array == 0 else cot_send).at[span(dest, capacity), :]
            return remote(source, piece(arrays[array], block, seat(which, core)),
                          ep_send.at[dest], ep_recv.at[min(i, 1), block], dest, tp)

        def bulk(block, count, send, recv):
            at = tok_rows.at[span(block, capacity), pl.ds(0, count * col)]
            return remote(at, at, send, recv, me, partner)

        def mix_copy(dest, block):
            return remote(mix_send.at[dest], mix_in.at[block], m_send.at[0], m_recv.at[block], dest, tp)

        def y_copy(array, step, block):
            at = piece(arrays[array], block, tp)
            return remote(at, at, y_send.at[block], y_recv.at[array, step - 1, block], me, seat(step, core))

        def y_arrival(array, step, block):
            at = piece(arrays[array], block, seat(-step, core))
            return remote(at, at, y_send.at[block], y_recv.at[array, step - 1, block], me, seat(step, core))

        def c_copy(array, step, block):
            at = piece(arrays[array], block, seat(step, core))
            return remote(at, at, c_send.at[block], c_recv.at[block], me, partner)

        inner = (my_chunk + my_chunk // 2) % 2

        def choose(s, values):
            return sum(jnp.where(s == i, v, 0) for i, v in enumerate(values))

        def order(s):
            if chunks != 4:
                return s
            return jnp.where(inner == 1, choose(s, (0, 1, 2, 3)), choose(s, (0, 2, 1, 3)))

        def take_order(s):
            if chunks != 4:
                return s
            return jnp.where(inner == 1, s, choose(s, (2, 0, 1, 3)))

        def send(lo, hi):
            def action(k):
                for i in range(lo, hi):
                    ep_copy(i, peer(k), me).start()

            return action

        def send_far(on):
            for s in range(half // per_chunk, chunks):
                start = s * per_chunk
                each(start, start + per_chunk * on, send(0, len(far)))

        c_copy(1, 0, me).start()
        each(1, half, send(0, len(near)))
        loads[2].wait()
        logits = dot(router_ref[...], tok_ref[...], NT)
        chosen_first = jnp.sum(jnp.where(is_first, logits, 0.0), axis=0, keepdims=True)
        chosen_second = jnp.sum(jnp.where(is_second, logits, 0.0), axis=0, keepdims=True)
        mix_first = 1.0 / (1.0 + jnp.exp(chosen_second - chosen_first))
        mix_second = 1.0 / (1.0 + jnp.exp(chosen_first - chosen_second))
        mix_value = jnp.where(is_first, mix_first, jnp.where(is_second, mix_second, 0.0)).astype(BF)
        for e in range(senders):
            mix_send[e, :, 0:capacity] = dot(mix_value, pick[e * capacity:(e + 1) * capacity, :], NT)
        mix_in[me] = mix_send[me]
        each(1, senders, lambda k: mix_copy(peer(k), me).start())
        send_far(inner)
        for step in range(1, rows):
            raw_copy(step).wait_recv()
            cot_more[step - 1] = dot(pick[span(my_chunk, chunk), :], cot_raw[step - 1]).astype(BF)
            cot_rows[own, span(seat(-step, core), col)] = cot_more[step - 1, span(me - close_first, capacity), :]
            c_copy(1, -step, me).start()
        each(1, per_chunk, send(len(near), len(close)))
        send_far(1 - inner)

        def take(items, hops):
            def action(j):
                block = peer(j)
                for i, (array, step) in enumerate(items):
                    if i == 0:
                        ep_copy(0, block, block).wait_recv()
                    if i == 1:
                        bulk(block, len(items) - 1, ep_send.at[block], ep_recv.at[1, block]).wait_recv()
                    for a, hop in hops:
                        if a == array and step == 0:
                            y_copy(array, hop, block).start()
                    c_copy(array, step, block).start()

            return action

        def pass_on(hops):
            def action(j):
                block = peer(j)
                for array, step in hops:
                    y_arrival(array, step, block).wait_recv()
                    c_copy(array, -step, block).start()

            return action

        def settle(items, hops):
            def action(j):
                block = peer(j)
                bulk(block, len(items) + len(hops), c_send.at[block], c_recv.at[block]).wait_recv()

            return action

        def arrive_mix(j):
            mix_copy(peer(j), peer(j)).wait_recv()

        def home_copy(dest, slot):
            return remote(piece(terms, dest, tp), home.at[span(slot, capacity), :],
                          h_send.at[0], h_recv.at[0], dest, tp)

        def part_copy(dest, slot):
            return remote(mp_send.at[dest], mp_got.at[slot], p_send.at[0], p_recv.at[0], dest, tp)

        def rc_copy(step, block):
            return remote(piece(terms, block, seat(step, 1 - core)), c_buf.at[step, span(block, capacity), :],
                          rc_send.at[block], rc_recv.at[step, block], me, partner)

        def ry_copy(step, block):
            return remote(piece(terms, block, seat(step, core)), y_buf.at[step - 1, span(block, capacity), :],
                          ry_send.at[block], ry_recv.at[step - 1, block], me, seat(step, core))

        def first(j):
            block = peer(j)
            at = span(block, capacity)
            for step in range(1, rows):
                rc_copy(step, block).wait_recv()
                cols = span(seat(step, core), col)
                terms[at, cols] = (terms[at, cols].astype(F32) + c_buf[step, at, :].astype(F32)).astype(BF)
                ry_copy(step, block).start()

        def second(j):
            block = peer(j)
            at = span(block, capacity)
            rc_copy(0, block).wait_recv()
            value = terms[at, span(tp, col)].astype(F32) + c_buf[0, at, :].astype(F32)
            for step in range(1, rows):
                ry_copy(step, block).wait_recv()
                value = value + y_buf[step - 1, at, :].astype(F32)
            terms[at, span(tp, col)] = value.astype(BF)

            @pl.when(j > 0)
            def _():
                home_copy(block, me).start()

        diagonal = lax.broadcasted_iota(jnp.int32, (capacity, capacity), 0) == lax.broadcasted_iota(
            jnp.int32, (capacity, capacity), 1)

        def to_column(values):
            return jnp.sum(jnp.where(diagonal, values, 0.0), axis=1, keepdims=True)

        def to_row(values):
            return jnp.sum(jnp.where(diagonal, values, 0.0), axis=0, keepdims=True)

        def forward(which):
            at = span(which, chunk)
            mixes = jnp.concatenate(
                [to_column(mix_in[which * per_chunk + i, pl.ds(me, 1), :][:, 0:capacity]) for i in range(per_chunk)],
                axis=0)
            x = tok_rows[at, :]
            dy = cot_rows[at, :]
            total = jnp.zeros((chunk, 1), F32)
            for n0 in range(0, hidden, CHUNK):
                n = min(CHUNK, hidden - n0)
                gate = dot(x, wg[:, n0:n0 + n])
                up = dot(x, wu[:, n0:n0 + n])
                back = dot(dy, wd[n0:n0 + n, :], NT)
                sig = 1.0 / (1.0 + jnp.exp(-gate))
                active = gate * sig
                inner = active * up
                total = total + jnp.sum(inner * back, axis=1, keepdims=True)
                scaled = mixes * back
                gb[at, n0:n0 + n] = (scaled * up * sig * (1.0 + gate * (1.0 - sig))).astype(BF)
                ub[at, n0:n0 + n] = (scaled * active).astype(BF)
                hs[at, n0:n0 + n] = (mixes * inner).astype(BF)
            for i in range(per_chunk):
                line = to_row(total[i * capacity:(i + 1) * capacity, :])
                mp_send[which * per_chunk + i, :, 0:capacity] = jnp.broadcast_to(line, (8, capacity))

        def backward(which, lo):
            at = span(which, chunk)
            gate_back = gb[at, :]
            up_back = ub[at, :]
            for step in list(range(1, rows)) + [0]:
                for side in (1 - core, core):
                    cols = span(seat(step, side), col)
                    terms[at, cols] = (dot(gate_back, wg[cols, :], NT) + dot(up_back, wu[cols, :], NT)).astype(BF)
                for i in range(per_chunk):
                    rc_copy(step, peer(lo + i)).start()

        def ranged(own_action, close_action, near_action, far_action):
            def run(lo, hi):
                if own_action is not None:
                    each(lo, jnp.minimum(hi, 1), own_action)
                if close_action is not None:
                    each(jnp.maximum(lo, 1), jnp.minimum(hi, per_chunk), close_action)
                each(jnp.maximum(lo, per_chunk), jnp.minimum(hi, half), near_action)
                each(jnp.maximum(lo, half), hi, far_action)

            return run

        take_range = ranged(None, take(close, []), take(near, near_hops), take(far, far_hops))
        pass_range = ranged(None, None, pass_on(near_hops), pass_on(far_hops))
        settle_range = ranged(settle(mine, []), settle(close, []), settle(near, near_hops), settle(far, far_hops))
        part = (per_chunk + 1) // 2

        def take_halves(lo, hi):
            def one(h):
                start = take_order(h // 2) * per_chunk + h % 2 * part
                take_range(start, start + part)

            each(lo, hi, one)

        def taken(s, point):
            def of(table):
                return choose(s, [table[3 * i + point] for i in range(4)])

            return jnp.where(inner == 1, of(INNER_TAKES), of(OUTER_TAKES))

        def take_point(s, point):
            take_halves(taken(s, point - 1), taken(s, point))

        take_halves(0, 4)

        def joined(ref, steps, cols):
            return jnp.concatenate([ref[span(pair(my_chunk, order(s), chunks), chunk), cols] for s in steps], axis=0)

        first_half, second_half = range(chunks // 2), range(chunks // 2, chunks)

        def down_early(i):
            at = span(i, LANES)
            x = joined(hs, range(chunks - 1), at)
            for n0 in range(0, width, 512):
                dg[at, n0:n0 + 512] = dot(x, joined(cot_rows, range(chunks - 1), slice(n0, n0 + 512)), TN).astype(BF)

        def down(i):
            at = span(i, LANES)
            x = joined(hs, [chunks - 1], at)
            for n0 in range(0, width, 512):
                more = dot(x, joined(cot_rows, [chunks - 1], slice(n0, n0 + 512)), TN)
                dg[at, n0:n0 + 512] = (dg[at, n0:n0 + 512].astype(F32) + more).astype(BF)

        def gate_up_early(i):
            at = span(i, CHUNK)
            x = joined(tok_rows, first_half, at)
            gg[at, :] = dot(x, joined(gb, first_half, slice(None)), TN).astype(BF)
            ug[at, :] = dot(x, joined(ub, first_half, slice(None)), TN).astype(BF)

        def gate_up(i):
            at = span(i, CHUNK)
            x = joined(tok_rows, second_half, at)
            gg[at, :] = (gg[at, :].astype(F32) + dot(x, joined(gb, second_half, slice(None)), TN)).astype(BF)
            ug[at, :] = (ug[at, :].astype(F32) + dot(x, joined(ub, second_half, slice(None)), TN)).astype(BF)

        cuts = [hidden // LANES * 3 // 7, hidden // LANES * 5 // 7, hidden // LANES]
        ready = width // CHUNK * 5 // 8

        def step_of(s):
            lo = order(s) * per_chunk
            hi = lo + per_chunk
            before = order(jnp.maximum(s - 1, 0)) * per_chunk
            earlier_chunk = order(jnp.maximum(s - 2, 0)) * per_chunk
            which = pair(my_chunk, order(s), chunks)

            each(0, jnp.where(s == chunks - 1, cuts[0], 0), down_early)
            pass_range(jnp.where(s == 2, hi, lo), hi)
            each(cuts[0], jnp.where(s == chunks - 1, cuts[1], cuts[0]), down_early)
            settle_range(lo, hi)
            each(jnp.maximum(lo, 1), hi, arrive_mix)

            @pl.when(s == 0)
            def _():
                for load in loads[4:]:
                    load.wait()

            forward(which)
            each(jnp.maximum(lo, 1), hi, lambda j: part_copy(peer(j), me).start())
            take_point(s, 1)
            each(earlier_chunk, earlier_chunk + jnp.where(s == 2, per_chunk, 0), second)
            each(before, before + jnp.where(s > 1, per_chunk, 0), second)
            backward(which, lo)
            each(lo, hi, first)
            take_point(s, 2)
            each(0, jnp.where(s == chunks // 2 - 1, ready, 0), gate_up_early)
            take_point(s, 3)
            coming = order(min(2, chunks - 1)) * per_chunk + per_chunk
            pass_range(jnp.where(s == 1, coming - per_chunk, coming), coming)
            each(ready, jnp.where(s == chunks // 2 - 1, width // CHUNK, ready), gate_up_early)

        each(0, chunks, step_of)
        mp_got[me] = mp_send[me]

        parts = width // CHUNK
        last = order(chunks - 1) * per_chunk
        middle = last + (per_chunk + 1) // 2
        each(0, parts // 2, gate_up)
        others = pl.ds(0, senders - 1)

        def all_parts():
            return remote(mp_send.at[others], mp_got.at[others], p_send.at[0], p_recv.at[0], me, partner)

        all_parts().wait_recv()
        mix_all[0] = mp_got[...]

        def t_copy(k):
            return remote(mp_got, mix_all.at[k], t_send.at[k], t_recv.at[k], me, lax.rem(tp + k, seats))

        for k in range(1, seats):
            t_copy(k).start()
        each(last, middle, second)
        each(parts // 2, parts * 3 // 4, gate_up)
        for k in range(1, seats):
            t_copy(k).wait()

        slot_mix = jnp.sum(mix_all[...], axis=0)
        grads = []
        for e in range(senders):
            column = to_column(slot_mix[e, 0:1, 0:capacity])
            chosen = pick[e * capacity:(e + 1) * capacity, :].astype(F32)
            grads.append(jnp.sum(column * chosen, axis=0, keepdims=True))
        grads = jnp.concatenate(grads, axis=0)
        mg_first = jnp.sum(jnp.where(is_first, grads, 0.0), axis=0, keepdims=True)
        mg_second = jnp.sum(jnp.where(is_second, grads, 0.0), axis=0, keepdims=True)
        mix_out[0:1, :] = mg_first
        mix_out[1:2, :] = mg_second
        lg_first = mix_first * mix_second * (mg_first - mg_second)
        route_grad = split(jnp.where(is_first, lg_first, jnp.where(is_second, -lg_first, 0.0)))
        raw = dot(route_grad, tok_ref[...])
        norm_scale = 1.0 / math.sqrt(home_rows * senders)
        rt_full[...] = (raw[0:senders] + raw[senders:2 * senders] + raw[2 * senders:]) * norm_scale

        def rt_cols(dest):
            return span((dest * seats + tp) * share // LANES, LANES)

        def r_copy(dest, slot):
            return remote(rt_full.at[:, rt_cols(dest)], rt_got.at[slot], r_send.at[0], r_recv.at[0], dest, tp)

        each(1, senders, lambda k: r_copy(peer(k), me).start())
        rt_got[me] = rt_full[:, rt_cols(me)]
        each(middle, last + per_chunk, second)
        each(parts * 3 // 4, parts, gate_up)
        each(cuts[1], cuts[2], down_early)
        each(0, hidden // LANES, down)

        def finish(items, hops):
            def action(j):
                block = peer(j)
                bulk(block, len(items) + len(hops), c_send.at[block], c_recv.at[block]).wait_send()
                if hops:
                    bulk(block, len(hops), y_send.at[block], y_recv.at[0, 0, block]).wait_send()
                if items is not mine:
                    bulk(block, len(items), ep_send.at[block], ep_recv.at[0, block]).wait_send()

            return action

        for step in range(1, rows):
            raw_copy(step).wait_send()
        finish(mine, [])(0)
        each(1, per_chunk, finish(close, []))
        each(per_chunk, half, finish(near, near_hops))
        each(half, senders, finish(far, far_hops))

        def close_back(j):
            block = peer(j)
            bulk(block, rows, rc_send.at[block], rc_recv.at[0, block]).wait_send()
            bulk(block, rows - 1, ry_send.at[block], ry_recv.at[0, block]).wait_send()

        each(0, senders, close_back)
        remote(mix_send.at[others], mix_in.at[others], m_send.at[0], m_recv.at[0], me, partner).wait_send()
        all_parts().wait_send()

        def all_home():
            at = home.at[pl.ds(0, (senders - 1) * capacity), :]
            return remote(at, at, h_send.at[0], h_recv.at[0], me, partner)

        def all_router():
            at = rt_got.at[others]
            return remote(at, at, r_send.at[0], r_recv.at[0], me, partner)

        home[own, :] = terms[own, span(tp, col)]
        all_home().wait_recv()
        cols = router_ref[:, span(tp, col)]
        tg_out[...] = (
            dot(pick[...], home[...], TN) + dot(route_grad, jnp.concatenate([cols, cols, cols], axis=0), TN)
        ).astype(BF)
        all_router().wait_recv()
        rt_out[...] = jnp.sum(rt_got[...], axis=0)
        all_home().wait_send()
        all_router().wait_send()

    return body


def layer(tokens, cotangent, routes, router, w_gate, w_up, w_down):
    home_rows, width = tokens.shape
    senders = router.shape[0]
    seats = lax.axis_size("tp")
    rows = seats // 2
    col = width // seats
    hidden = w_gate.shape[1]
    capacity = home_rows * routes.shape[0] * 2 // senders
    slots = senders * capacity
    share = width // (senders * seats)
    vmem = pl.BlockSpec(memory_space=pltpu.VMEM)
    hbm = pl.BlockSpec(memory_space=pltpu.HBM)
    dma = pltpu.SemaphoreType.DMA

    def buf(shape, dtype=BF):
        return pltpu.VMEM(shape, dtype)

    return pl.pallas_call(
        layer_kernel(senders, rows, capacity, col, hidden, share),
        out_shape=(
            buf((home_rows, col)),
            buf((2, home_rows), F32),
            buf((senders, LANES), F32),
            buf((width, hidden)),
            buf((width, hidden)),
            buf((hidden, width)),
        ),
        in_specs=[hbm] * 7,
        out_specs=[vmem] * 6,
        scratch_shapes=[
            buf(tokens.shape), buf(cotangent.shape), buf(routes.shape, routes.dtype), buf(router.shape),
            buf((width, hidden)), buf((width, hidden)), buf((hidden, width)),
            buf((slots, home_rows)), buf((rows, slots, col)), buf((slots, col)),
            buf((rows - 1, home_rows, col)), buf((rows - 1, max(CHUNK, capacity), col)),
            buf((senders, senders, LANES), F32), buf((senders, senders, LANES), F32),
            buf((slots, width)), buf((slots, width)),
            buf((slots, hidden)), buf((slots, hidden)), buf((slots, hidden)), buf((slots, width)),
            buf((senders, 8, LANES), F32), buf((senders, 8, LANES), F32), buf((seats, senders, 8, LANES), F32),
            buf((rows, slots, col)), buf((rows - 1, slots, col)), buf((slots, col)),
            buf((senders, width), F32), buf((senders, senders, LANES), F32),
            dma((7,)), dma((rows - 1,)), dma((rows - 1,)),
            dma((senders,)), dma((2, senders)),
            dma((senders,)), dma((2, rows - 1, senders)),
            dma((senders,)), dma((senders,)),
            dma((1,)), dma((senders,)),
            dma((senders,)), dma((rows, senders)),
            dma((senders,)), dma((rows - 1, senders)),
            dma((1,)), dma((1,)),
            dma((1,)), dma((1,)),
            dma((seats,)), dma((seats,)),
            dma((1,)), dma((1,)),
        ],
        compiler_params=pltpu.CompilerParams(has_side_effects=True, collective_id=0, vmem_limit_bytes=46 << 20),
        name="layer",
    )(tokens, cotangent, routes, router, w_gate, w_up, w_down)


def output_kernel(share):
    def body(tg, mix, rt, gg, ug, dg, tg_out, mix_out, rt_out, gg_out, ug_out, dg_out, sem):
        copies = [pltpu.make_async_copy(src, dst, sem.at[i])
                  for i, (src, dst) in enumerate(((gg, gg_out), (ug, ug_out), (dg, dg_out), (tg, tg_out), (mix, mix_out)))]
        for copy in copies:
            copy.start()
        offset = (lax.axis_index("ep") * lax.axis_size("tp") + lax.axis_index("tp")) * share % LANES
        total = jnp.zeros(rt_out.shape, F32)
        for start in range(0, LANES, share):
            total = total + jnp.where(offset == start, rt[:, start:start + share], 0.0)
        rt_out[...] = total
        for copy in copies:
            copy.wait()

    return body


def outputs(token_grad, mixing, router_rows, gate_grad, up_grad, down_grad, share):
    vmem = pl.BlockSpec(memory_space=pltpu.VMEM)
    hbm = pl.BlockSpec(memory_space=pl.ANY)
    like = [jax.ShapeDtypeStruct(x.shape, x.dtype) for x in (token_grad, mixing, router_rows, gate_grad, up_grad, down_grad)]
    like[2] = jax.ShapeDtypeStruct((router_rows.shape[0], share), F32)
    return pl.pallas_call(
        output_kernel(share),
        out_shape=like,
        in_specs=[vmem] * 6,
        out_specs=[hbm, hbm, vmem, hbm, hbm, hbm],
        scratch_shapes=[pltpu.SemaphoreType.DMA((5,))],
        compiler_params=pltpu.CompilerParams(vmem_limit_bytes=4 << 20),
        name="outputs",
    )(token_grad, mixing, router_rows, gate_grad, up_grad, down_grad)


def local(tokens, routes, router_matrix, cotangent, gate_proj, up_proj, down_proj):
    share = tokens.shape[1] // (lax.axis_size("ep") * lax.axis_size("tp"))
    results = layer(
        tokens, cotangent, routes.T, router_matrix.T, gate_proj[0], up_proj[0], down_proj[0]
    )
    token_grad, mixing, router_grad, gate_grad, up_grad, down_grad = outputs(*results, share)
    return (token_grad, mixing.T, router_grad.T, gate_grad[None], up_grad[None], down_grad[None])


def solution(mesh):
    return jax.shard_map(
        local,
        mesh=mesh,
        in_specs=(
            P("ep", None),
            P("ep", None),
            P(),
            P("ep", "tp"),
            P("ep", None, "tp"),
            P("ep", None, "tp"),
            P("ep", "tp", None),
        ),
        out_specs=(
            P("ep", "tp"),
            P("ep", None),
            P(("ep", "tp"), None),
            P("ep", None, "tp"),
            P("ep", None, "tp"),
            P("ep", "tp", None),
        ),
        check_vma=False,
    )
```
